512 devices in a mesh: sp: 64 (over z, y), tp: 8 (over x, core).
Axes of the slice: x: 4, y: 4, z: 16, core: 2. Of those that a mesh axis runs over, the one named last changes fastest.
Arguments:
- tokens: bfloat16 [24576, 4096], P(('sp', 'tp')), may hold values from -6 to 6
- norm_gain: float32 [4096], replicated, may hold values from 0.1 to 1.9
- conv_val_w: bfloat16 [4096, 1024], P('sp', 'tp'), may hold values from -0.09375 to 0.09375
- conv_gate_w: bfloat16 [4096, 1024], P('sp', 'tp'), may hold values from -0.09375 to 0.09375
- rec_gate_w: bfloat16 [4096, 1536], P('sp', 'tp'), may hold values from -0.09375 to 0.09375
- rec_in_w: bfloat16 [4096, 1536], P('sp', 'tp'), may hold values from -0.09375 to 0.09375
- conv_taps: bfloat16 [31, 1024], P(None, 'tp'), may hold values from -3 to 3
- conv_bias: float32 [1024], P('tp'), may hold values from 1 to 15
- conv_gain: float32 [1024], P('tp'), may hold values from 0.1 to 1.9
- short_taps: bfloat16 [4, 1536], P(None, 'tp'), may hold values from -3 to 3
- decay_map: bfloat16 [24, 64, 64], P('tp'), may hold values from -0.75 to 0.75
- input_map: bfloat16 [24, 64, 64], P('tp'), may hold values from -0.75 to 0.75
- decay_base: float32 [1536], P('tp'), may hold values from 3.5 to 17
- decay_jump: float32 [24576, 1536], P('sp', 'tp'), may hold values from -1.5 to 0
- out_conv_w: bfloat16 [1024, 4096], P('tp', 'sp'), may hold values from -0.125 to 0.125
- out_rec_w: bfloat16 [1536, 4096], P('tp', 'sp'), may hold values from -0.125 to 0.125
Outputs:
- mixed: bfloat16 [24576, 4096], P(('sp', 'tp'))
The draws below stay inside these ranges and needn't reach their ends.
All inputs are finite; a program needn't handle non-finite values.
Results may differ from the reference program's by a relative error of at most 0.015.
Values may be sent and summed in bfloat16 or wider, within the bound.
A program may use at most 64 MiB of HBM per device.

```python
import math
import jax
import jax.numpy as jnp
from jax import lax

D = 4096
HEAD_SIZE = 64
LRU_HEADS = 24
TAPS = 31
SHORT_TAPS = 4
CONV_WIDTH = 1024
LRU_WIDTH = 1536
TOKENS = 24576
N_TP = 8


def draw_conv_taps(key, part):
    key_base, key_jitter = jax.random.split(jax.random.fold_in(key, 31))
    channel = jnp.arange(CONV_WIDTH, dtype=jnp.float32) / CONV_WIDTH
    jitter = jnp.exp(jax.random.uniform(key_jitter, (CONV_WIDTH,), jnp.float32, math.log(0.8), math.log(1.25)))
    base = jnp.clip(jax.random.normal(key_base, (TAPS, CONV_WIDTH), jnp.float32), -4.0, 4.0)
    rising = jnp.exp(math.log(3.0) * channel)
    return (base * (rising * jitter)[None, :] * (1.0 / math.sqrt(TAPS))).astype(jnp.bfloat16)


def draw_conv_bias(key, part):
    key_jitter = jax.random.fold_in(key, 37)
    channel = jnp.arange(CONV_WIDTH, dtype=jnp.float32) / CONV_WIDTH
    jitter = jnp.exp(jax.random.uniform(key_jitter, (CONV_WIDTH,), jnp.float32, math.log(0.8), math.log(1.25)))
    rising = jnp.exp(math.log(4.0) * channel)
    return 1.5 * rising * jitter


def draw_decay_base(key, part):
    key_kind, key_slow, key_fast = jax.random.split(jax.random.fold_in(key, 29), 3)
    keep_share = 0.5
    slow = jax.random.uniform(key_kind, (LRU_WIDTH,), jnp.float32) < keep_share
    slow_rate = jnp.exp(jax.random.uniform(key_slow, (LRU_WIDTH,), jnp.float32, math.log(0.01), math.log(0.05))) / TOKENS
    fast_rate = jnp.exp(jax.random.uniform(key_fast, (LRU_WIDTH,), jnp.float32, math.log(0.0075), math.log(0.025)))
    rate = jnp.where(slow, slow_rate, fast_rate)
    return -jnp.log(jnp.expm1(rate))


def draw_decay_jump(key, part):
    key_leak, key_where, key_drop = jax.random.split(jax.random.fold_in(key, 23), 3)
    blocks = (TOKENS + 63) // 64
    lowest, highest = (0.05, 0.5)
    leak = jnp.exp(jax.random.uniform(key_leak, (blocks,), jnp.float32, math.log(lowest), math.log(highest))) / TOKENS
    position_leak = jnp.repeat(leak, 64)[:TOKENS]
    places = jax.random.randint(key_where, (2,), 0, TOKENS)
    hits = (jnp.arange(TOKENS)[:, None] == places[None, :]).astype(jnp.float32)
    drops = jnp.log1p(-jax.random.uniform(key_drop, (2, LRU_WIDTH), jnp.float32, 0.2, 0.5))
    return jnp.dot(hits, drops, precision=lax.Precision.HIGHEST) - position_leak[:, None]


def block_levels(stream_key, shape, pieces, low, high):
    level = 1.0
    for axis_at, blocks in pieces:
        heights = jax.random.uniform(jax.random.fold_in(jax.random.fold_in(stream_key, 6), axis_at), (blocks,), jnp.float32, low / len(pieces), high / len(pieces))
        level = level * jnp.repeat(jnp.exp(heights), shape[axis_at] // blocks).reshape((-1,) + (1,) * (len(shape) - 1 - axis_at))
    return level


def gaussian(key, shape, width, most, pieces=(), kind=jnp.bfloat16):
    level = block_levels(key, shape, pieces, -0.22, 0.18) if pieces else 1.0
    drawn = jax.random.normal(key, shape, jnp.float32) * width * level
    return jnp.minimum(jnp.maximum(drawn, -most), most).astype(kind)


def setup_inputs(seed: int = 0) -> dict:
    key_list = jax.random.split(jax.random.key(seed), 17)
    return {
        "tokens": gaussian(key_list[0], (TOKENS, D), 1.0, 6.0, ((0, 512),)),
        "norm_gain": jnp.clip(1.0 + 0.18 * jax.random.normal(key_list[1], (D,), jnp.float32), 0.1, 1.9),
        "conv_val_w": gaussian(key_list[2], (D, CONV_WIDTH), D ** -0.5, 0.09375, ((0, 64), (1, 8))),
        "conv_gate_w": gaussian(key_list[3], (D, CONV_WIDTH), D ** -0.5, 0.09375, ((0, 64), (1, 8))),
        "rec_gate_w": gaussian(key_list[4], (D, LRU_WIDTH), D ** -0.5, 0.09375, ((0, 64), (1, 8))),
        "rec_in_w": gaussian(key_list[5], (D, LRU_WIDTH), D ** -0.5, 0.09375, ((0, 64), (1, 8))),
        "conv_taps": draw_conv_taps(jax.random.fold_in(key_list[16], 71), 0),
        "conv_bias": draw_conv_bias(jax.random.fold_in(key_list[16], 71), 0),
        "conv_gain": jnp.clip(1.0 + 0.18 * jax.random.normal(key_list[8], (CONV_WIDTH,), jnp.float32), 0.1, 1.9),
        "short_taps": gaussian(key_list[9], (SHORT_TAPS, LRU_WIDTH), SHORT_TAPS ** -0.5, 3.0, ((1, 8),)),
        "decay_map": gaussian(key_list[10], (LRU_HEADS, HEAD_SIZE, HEAD_SIZE), HEAD_SIZE ** -0.5, 0.75, ((0, 8),)),
        "input_map": gaussian(key_list[11], (LRU_HEADS, HEAD_SIZE, HEAD_SIZE), HEAD_SIZE ** -0.5, 0.75, ((0, 8),)),
        "decay_base": draw_decay_base(jax.random.fold_in(key_list[16], 71), 0),
        "decay_jump": draw_decay_jump(jax.random.fold_in(key_list[16], 71), 0),
        "out_conv_w": gaussian(key_list[14], (CONV_WIDTH, D), (CONV_WIDTH + LRU_WIDTH) ** -0.5, 0.125, ((0, 8), (1, 64))),
        "out_rec_w": gaussian(key_list[15], (LRU_WIDTH, D), (CONV_WIDTH + LRU_WIDTH) ** -0.5, 0.125, ((0, 8), (1, 64))),
    }


RATE_SCALE = 8.0

def norm_rows(values, gain):
    widened = values.astype(jnp.float32)
    inverse = lax.rsqrt(lax.optimization_barrier(jnp.mean(widened * widened, axis=-1, keepdims=True)) + 1e-06)
    return (widened * inverse * gain).astype(jnp.bfloat16)

def causal_filter(signal, weights):
    lags = weights.shape[0]
    length = signal.shape[0]
    padded = jnp.pad(signal, ((lags - 1, 0), (0, 0)))
    result = jnp.zeros_like(signal)
    for lag_index in range(lags):
        result = result + weights[lag_index][None, :] * padded[lag_index:lag_index + length]
    return result

def chain_step(earlier, latter):
    return (earlier[0] * latter[0], latter[0] * earlier[1] + latter[1])

def reference(tokens, norm_gain, conv_val_w, conv_gate_w, rec_gate_w, rec_in_w, conv_taps, conv_bias, conv_gain, short_taps, decay_map, input_map, decay_base, decay_jump, out_conv_w, out_rec_w):
    normed = norm_rows(tokens, norm_gain)
    conv_val = jnp.dot(normed, conv_val_w, preferred_element_type=jnp.float32).astype(jnp.bfloat16)
    conv_gate = jnp.dot(normed, conv_gate_w, preferred_element_type=jnp.float32).astype(jnp.bfloat16)
    rec_gate = jnp.dot(normed, rec_gate_w, preferred_element_type=jnp.float32).astype(jnp.bfloat16)
    rec_in = jnp.dot(normed, rec_in_w, preferred_element_type=jnp.float32).astype(jnp.bfloat16)
    glu = (conv_val.astype(jnp.float32) * jax.nn.sigmoid(conv_gate.astype(jnp.float32))).astype(jnp.bfloat16)
    filtered = causal_filter(glu.astype(jnp.float32), conv_taps.astype(jnp.float32)) + conv_bias[None, :]
    centered = filtered - lax.optimization_barrier(jnp.mean(filtered, axis=1, keepdims=True))
    spread = lax.optimization_barrier(jnp.mean(centered * centered, axis=1, keepdims=True))
    conv_out = jax.nn.silu(centered * lax.rsqrt(spread + 1e-05) * conv_gain).astype(jnp.bfloat16)
    smoothed = causal_filter(rec_in.astype(jnp.float32), short_taps.astype(jnp.float32)).astype(jnp.bfloat16)
    grouped = smoothed.astype(jnp.float32).reshape(TOKENS, LRU_HEADS, HEAD_SIZE)
    retain = jax.nn.sigmoid(jnp.einsum('thi,hio->tho', grouped, decay_map.astype(jnp.float32)).reshape(TOKENS, LRU_WIDTH))
    admit = jax.nn.sigmoid(jnp.einsum('thi,hio->tho', grouped, input_map.astype(jnp.float32)).reshape(TOKENS, LRU_WIDTH))
    log_decay = -RATE_SCALE * retain * jax.nn.softplus(-decay_base)[None, :] + decay_jump
    decay = jnp.exp(log_decay)
    inflow = jnp.sqrt(-jnp.expm1(2.0 * log_decay)) * admit * smoothed.astype(jnp.float32)
    products, state = lax.associative_scan(chain_step, (decay, inflow), axis=0)
    rec_out = (jax.nn.gelu(rec_gate.astype(jnp.float32)) * state).astype(jnp.bfloat16)
    conv_block = CONV_WIDTH // N_TP
    rec_block = LRU_WIDTH // N_TP
    mixed = jnp.zeros((TOKENS, D), jnp.float32)
    for block_index in range(N_TP):
        conv_cols = slice(block_index * conv_block, (block_index + 1) * conv_block)
        rec_cols = slice(block_index * rec_block, (block_index + 1) * rec_block)
        term = jnp.dot(conv_out[:, conv_cols], out_conv_w[conv_cols], preferred_element_type=jnp.float32)
        term = term + jnp.dot(rec_out[:, rec_cols], out_rec_w[rec_cols], preferred_element_type=jnp.float32)
        mixed = mixed + lax.optimization_barrier(term.astype(jnp.bfloat16)).astype(jnp.float32)
    return mixed.astype(jnp.bfloat16)
```

```python
import jax
import jax.numpy as jnp
from jax import lax
from jax.experimental import pallas as pl
from jax.experimental.pallas import tpu as pltpu
from jax.sharding import PartitionSpec as P

MESH = pl.DeviceIdType.MESH
CONV_WIDTH = 1024
RATE_SCALE = 8.0
NZ, NY, NX, NC = 16, 4, 4, 2
HALF = NZ // 2


def rem(a, n):
    return lax.rem(a + 4 * n, n)


class Gather:
    def __init__(self, a, b, rows, sems, pos):
        self.a, self.b, self.rows = a, b, rows
        self.s, self.r = sems[: len(sems) // 2], sems[len(sems) // 2 :]
        self.z, self.y = pos
        self.sent = []

    def at(self, ref, z, y):
        rows = self.rows
        return ref.at[pl.ds(pl.multiple_of((rem(z, NZ) * NY + rem(y, NY)) * rows, rows), rows)]

    def copy(self, ref, chunk, kind, index, to):
        block = self.at(ref, *chunk)
        return pltpu.make_async_remote_copy(
            src_ref=block,
            dst_ref=block,
            send_sem=self.s[kind].at[index],
            recv_sem=self.r[kind].at[index],
            device_id={"sp": rem(to[0], NZ) * NY + rem(to[1], NY)},
            device_id_type=MESH,
        )

    def send(self, *args):
        self.copy(*args).start()
        self.sent.append(args)

    def arrived(self, ref, chunk, kind, index):
        self.copy(ref, chunk, kind, index, (self.z + 1, self.y)).wait_recv()

    def start(self):
        z, y, a, b = self.z, self.y, self.a, self.b
        self.send(b, (z, y), 3, 0, (z + 1, y))
        self.send(b, (z, y), 4, 0, (z - 1, y))
        self.send(a, (z, y), 0, 0, (z, y + 1))
        self.send(a, (z, y), 0, 2, (z, y + 3))
        self.send(a, (z, y), 0, 1, (z, y + 2))
        self.send(a, (z, y), 1, 0, (z + 1, y))
        self.send(a, (z, y), 2, 0, (z - 1, y))
        self.spread(0)

    def start_y(self):
        z, y, a = self.z, self.y, self.a
        for d in (1, 3, 2):
            self.arrived(a, (z, y - d), 0, d - 1)
            self.send(a, (z, y - d), 1, d, (z + 1, y))
            self.send(a, (z, y - d), 2, d, (z - 1, y))

    def spread(self, k):
        z, y = self.z, self.y
        self.send(self.b, (z - k, y), 5, 3 * k, (z, y + 1))
        self.send(self.b, (z - k, y), 5, 3 * k + 1, (z, y - 1))

    def along_z(self, s):
        z, y, a, b = self.z, self.y, self.a, self.b
        self.arrived(b, (z - s, y), 3, s - 1)
        if s < HALF:
            self.send(b, (z - s, y), 3, s, (z + 1, y))
            self.arrived(b, (z + s, y), 4, s - 1)
            if s < HALF - 1:
                self.send(b, (z + s, y), 4, s, (z - 1, y))
            self.spread(s)
            self.spread(NZ - s)
        else:
            self.spread(s)
        for d in (0, 1, 3, 2):
            self.arrived(a, (z - s, y - d), 1, 4 * (s - 1) + d)
            if s < HALF:
                self.send(a, (z - s, y - d), 1, 4 * s + d, (z + 1, y))
                self.arrived(a, (z + s, y - d), 2, 4 * (s - 1) + d)
                if s < HALF - 1:
                    self.send(a, (z + s, y - d), 2, 4 * s + d, (z - 1, y))

    def along_y(self, k):
        z, y = self.z, self.y
        turn = 1 - 2 * (k % 2)
        self.arrived(self.b, (z - k, y - 1), 5, 3 * k)
        self.arrived(self.b, (z - k, y + 1), 5, 3 * k + 1)
        self.send(self.b, (z - k, y - turn), 5, 3 * k + 2, (z, y + turn))

    def along_y_last(self, k):
        self.arrived(self.b, (self.z - k, self.y + 2), 5, 3 * k + 2)

    def finish(self):
        for args in self.sent:
            self.copy(*args).wait_send()

    @staticmethod
    def semaphores():
        counts = [3, 4 * HALF, 4 * HALF, HALF, HALF, 3 * NZ]
        return [pltpu.SemaphoreType.DMA((n,)) for n in counts + counts]


N_SEMS = 12


def groups_of(step):
    if step == 0:
        return [0]
    if step < HALF:
        return [step, NZ - step]
    return [step] if step == HALF else []


def first_kernel(tokens, gain, wc_own, wr_own, oc_own, or_own, proj, oc, orr, *scratch):
    nt, wc, wr, acc_c, acc_r = scratch[:5]
    sems_in, sems_out = scratch[5 : 5 + N_SEMS], scratch[5 + N_SEMS : 5 + 2 * N_SEMS]
    tok_s, tok_r = scratch[5 + 2 * N_SEMS :]
    sp, tp = lax.axis_index("sp"), lax.axis_index("tp")
    z, y, x, c = sp // NY, sp % NY, tp // NC, tp % NC
    rows = wc_own.shape[0]
    n_tok = tokens.shape[0]
    width = tokens.shape[1]

    barrier = pltpu.get_barrier_semaphore()
    for dz, dy in ((1, 0), (-1, 0), (0, 1), (0, 2), (0, 3)):
        pl.semaphore_signal(
            barrier, inc=1, device_id={"sp": rem(z + dz, NZ) * NY + rem(y + dy, NY)}, device_id_type=MESH
        )
    for dx, dc in ((0, 1), (1, 0), (-1, 0)):
        pl.semaphore_signal(
            barrier, inc=1, device_id={"tp": rem(x + dx, NX) * NC + rem(c + dc, NC)}, device_id_type=MESH
        )

    own = pl.ds(pl.multiple_of(sp * rows, rows), rows)
    wc[own] = wc_own[...]
    wr[own] = wr_own[...]
    oc[own] = oc_own[...]
    orr[own] = or_own[...]
    pl.semaphore_wait(barrier, 8)

    g_in = Gather(wc, wr, rows, sems_in, (z, y))
    g_out = Gather(oc, orr, rows, sems_out, (z, y))
    g_in.start()

    def tok_at(xx, cc, lanes=None):
        r = pl.ds(pl.multiple_of((rem(xx, NX) * NC + rem(cc, NC)) * n_tok, 16), n_tok)
        return nt.at[r] if lanes is None else nt.at[r, lanes]

    def tok_copy(block, index, xx, cc):
        return pltpu.make_async_remote_copy(
            src_ref=block, dst_ref=block, send_sem=tok_s.at[index], recv_sem=tok_r.at[index],
            device_id={"tp": rem(xx, NX) * NC + rem(cc, NC)}, device_id_type=MESH,
        )

    t_sent = []

    def tok_send(*args):
        tok_copy(*args).start()
        t_sent.append(args)

    lo, hi = pl.ds(0, width // 2), pl.ds(width // 2, width // 2)

    widened = tokens[...].astype(jnp.float32)
    inverse = lax.rsqrt(jnp.mean(widened * widened, axis=-1, keepdims=True) + 1e-06)
    tok_at(x, c)[...] = (widened * inverse * gain[...]).astype(jnp.bfloat16)
    tok_send(tok_at(x, c), 0, x + 1, c)
    tok_send(tok_at(x, c), 1, x - 1, c)
    tok_send(tok_at(x, c), 4, x, c + 1)
    g_in.start_y()
    acc_c[...] = jnp.zeros_like(acc_c)
    acc_r[...] = jnp.zeros_like(acc_r)

    def tokens_forward():
        tok_copy(tok_at(x - 1, c), 0, x + 1, c).wait_recv()
        tok_send(tok_at(x - 1, c, lo), 2, x + 1, c)
        tok_send(tok_at(x - 1, c), 5, x, c + 1)
        tok_copy(tok_at(x + 1, c), 1, x + 1, c).wait_recv()
        tok_send(tok_at(x + 1, c, hi), 3, x - 1, c)
        tok_send(tok_at(x + 1, c), 6, x, c + 1)

    def tokens_last():
        tok_copy(tok_at(x + 2, c, lo), 2, x + 1, c).wait_recv()
        tok_send(tok_at(x + 2, c, lo), 7, x, c + 1)
        tok_copy(tok_at(x + 2, c, hi), 3, x + 1, c).wait_recv()
        tok_send(tok_at(x + 2, c, hi), 8, x, c + 1)
        tok_copy(tok_at(x, c + 1), 4, x + 1, c).wait_recv()
        tok_copy(tok_at(x - 1, c + 1), 5, x + 1, c).wait_recv()
        tok_copy(tok_at(x + 1, c + 1), 6, x + 1, c).wait_recv()
        tok_copy(tok_at(x + 2, c + 1, lo), 7, x + 1, c).wait_recv()
        tok_copy(tok_at(x + 2, c + 1, hi), 8, x + 1, c).wait_recv()

    def multiply(acc, w, first, count):
        def body(i, carry):
            cols = pl.ds(pl.multiple_of(rem(z - first - i, NZ) * (NY * rows), NY * rows), NY * rows)
            acc[...] += jnp.dot(nt[:, cols], w[cols, :], preferred_element_type=jnp.float32)
            return carry

        lax.fori_loop(0, count, body, 0)

    def multiply_runs(acc, w, steps):
        ks = sorted(k for s in steps for k in groups_of(s))
        runs = []
        for k in ks:
            if runs and runs[-1][0] + runs[-1][1] == k:
                runs[-1][1] += 1
            else:
                runs.append([k, 1])
        for first, count in runs:
            multiply(acc, w, first, count)

    go = 5
    for step in range(1, HALF + 3):
        if step == 2:
            g_out.start()
        if step <= HALF:
            g_in.along_z(step)
        if step == 3:
            g_out.start_y()
        if 2 < step:
            if step - 2 <= HALF:
                g_out.along_z(step - 2)
        for k in groups_of(step - 1):
            g_in.along_y(k)
        if step >= 2:
            for k in groups_of(step - 2):
                g_in.along_y_last(k)
        if step >= 4:
            for k in groups_of(step - 3):
                g_out.along_y(k)
        elif step == 3:
            g_out.along_y(0)
        if step == 3:
            tokens_forward()
        if step == go:
            tokens_last()
            multiply_runs(acc_c, wc, range(0, step + 1))
            multiply_runs(acc_r, wr, range(0, step - 1))
        elif step > go:
            multiply_runs(acc_c, wc, [step])
            multiply_runs(acc_r, wr, [step - 2])
    width_c = wc.shape[1]
    proj[:, :width_c] = acc_c[...].astype(jnp.bfloat16)
    proj[:, width_c:] = acc_r[...].astype(jnp.bfloat16)
    for k in groups_of(HALF):
        g_out.along_y(k)
    for k in range(NZ):
        g_out.along_y_last(k)
    g_in.finish()
    g_out.finish()
    for args in t_sent:
        tok_copy(*args).wait_send()


def passed_along(value, axis, by):
    count = lax.axis_size(axis)
    pairs = [(i, i + by) for i in range(count) if 0 <= i + by < count]
    return lax.ppermute(value, axis, pairs)


def sent_to_all(value, axis):
    count = lax.axis_size(axis)
    return lax.all_to_all(
        jnp.broadcast_to(value[None], (count, *value.shape)), axis, 0, 0, tiled=True
    )


def of_everyone(value, axis):
    return sent_to_all(value, axis).sum(axis=0)


def together(arrays, axis):
    ends = [0]
    for a in arrays:
        ends.append(ends[-1] + a.size)
    so_far = of_everyone(jnp.concatenate([a.ravel() for a in arrays]), axis)
    return tuple((so_far[b:e].reshape(a.shape) for a, b, e in zip(arrays, ends, ends[1:])))


def folded_in_pairs(pieces, combine):
    while len(jax.tree.leaves(pieces)[0]) > 1:
        pieces = jax.vmap(combine)(
            *(jax.tree.map(lambda part: part[side::2], pieces) for side in (0, 1))
        )
    return jax.tree.map(lambda part: part[0], pieces)


def carried_in(value, axis, combine, identity):
    count, mine = (lax.axis_size(axis), lax.axis_index(axis))
    passed = jnp.arange(count) < mine

    def kept(part, zero, own):
        return jnp.where(
            passed.reshape(-1, *(1 for _ in own.shape)), part, jnp.asarray(zero, own.dtype)
        )

    both = sent_to_all(jnp.stack(value), axis)
    pieces = (both[:, 0], both[:, 1])
    return folded_in_pairs(jax.tree.map(kept, pieces, identity, value), combine)


def causal_window(edge, current, weights):
    extended = jnp.concatenate([edge, current], axis=0).astype(jnp.float32)
    taps_wide = weights.astype(jnp.float32)
    length = current.shape[0]
    result = jnp.zeros((length, current.shape[1]), jnp.float32)
    for lag_index in range(weights.shape[0]):
        result = result + taps_wide[lag_index][None, :] * extended[lag_index : lag_index + length]
    return result


def chain_step(earlier, latter):
    return (earlier[0] * latter[0], latter[0] * earlier[1] + latter[1])


def glu_of(conv_val, conv_gate):
    return (conv_val.astype(jnp.float32) * jax.nn.sigmoid(conv_gate.astype(jnp.float32))).astype(
        jnp.bfloat16
    )


def shards(
    tokens, norm_gain, conv_val_w, conv_gate_w, rec_gate_w, rec_in_w, conv_taps, conv_bias, conv_gain,
    short_taps, decay_map, input_map, decay_base, decay_jump, out_conv_w, out_rec_w,
):
    conv_cols = conv_val_w.shape[1]
    rec_cols = rec_in_w.shape[1]
    conv_lags = conv_taps.shape[0] - 1
    short_lags = short_taps.shape[0] - 1
    n_tp, n_sp = lax.axis_size("tp"), lax.axis_size("sp")
    n_tok, width = tokens.shape
    rec_pad = -rec_cols % 128
    vmem = pl.BlockSpec(memory_space=pltpu.VMEM)
    projected, conv_full, rec_full = pl.pallas_call(
        first_kernel,
        out_shape=(
            jax.ShapeDtypeStruct((n_tok * n_tp, 2 * conv_cols + 2 * rec_cols), jnp.bfloat16),
            jax.ShapeDtypeStruct((width, conv_cols), jnp.bfloat16),
            jax.ShapeDtypeStruct((width, rec_cols + rec_pad), jnp.bfloat16),
        ),
        in_specs=[vmem] * 6,
        out_specs=(vmem,) * 3,
        scratch_shapes=[
            pltpu.VMEM((n_tok * n_tp, width), jnp.bfloat16),
            pltpu.VMEM((width, 2 * conv_cols), jnp.bfloat16),
            pltpu.VMEM((width, 2 * rec_cols), jnp.bfloat16),
            pltpu.VMEM((n_tok * n_tp, 2 * conv_cols), jnp.float32),
            pltpu.VMEM((n_tok * n_tp, 2 * rec_cols), jnp.float32),
            *Gather.semaphores(),
            *Gather.semaphores(),
            pltpu.SemaphoreType.DMA((9,)),
            pltpu.SemaphoreType.DMA((9,)),
        ],
        compiler_params=pltpu.CompilerParams(
            collective_id=0, has_side_effects=True, vmem_limit_bytes=60 * 1024 * 1024
        ),
    )(
        tokens,
        norm_gain[None, :],
        jnp.concatenate([conv_val_w, conv_gate_w], axis=1),
        jnp.concatenate([rec_gate_w, rec_in_w], axis=1),
        out_conv_w.T,
        jnp.pad(out_rec_w.T, ((0, 0), (0, rec_pad))),
    )
    glu = glu_of(projected[:, :conv_cols], projected[:, conv_cols : 2 * conv_cols])
    rec_gate = projected[:, 2 * conv_cols : 2 * conv_cols + rec_cols]
    rec_in = projected[:, 2 * conv_cols + rec_cols :]
    conv_edge, rec_edge = passed_along((glu[-conv_lags:], rec_in[-short_lags:]), "sp", 1)
    filtered = causal_window(conv_edge, glu, conv_taps) + conv_bias[None, :]
    row_total, row_squares = together(
        (jnp.sum(filtered, axis=1), jnp.sum(filtered * filtered, axis=1)), "tp"
    )
    row_mean = row_total / CONV_WIDTH
    spread = row_squares / CONV_WIDTH - row_mean * row_mean
    centered = filtered - row_mean[:, None]
    conv_out = jax.nn.silu(centered * lax.rsqrt(spread + 1e-05)[:, None] * conv_gain).astype(
        jnp.bfloat16
    )
    smoothed = causal_window(rec_edge, rec_in, short_taps).astype(jnp.bfloat16)
    length = smoothed.shape[0]
    grouped = smoothed.reshape(length, decay_map.shape[0], decay_map.shape[1])
    retain = jax.nn.sigmoid(
        jnp.einsum("thi,hio->tho", grouped, decay_map, preferred_element_type=jnp.float32).reshape(
            length, rec_cols
        )
    )
    admit = jax.nn.sigmoid(
        jnp.einsum("thi,hio->tho", grouped, input_map, preferred_element_type=jnp.float32).reshape(
            length, rec_cols
        )
    )
    log_decay = -RATE_SCALE * retain * jax.nn.softplus(-decay_base)[None, :] + decay_jump
    decay = jnp.exp(log_decay)
    inflow = jnp.sqrt(-jnp.expm1(2.0 * log_decay)) * admit * smoothed.astype(jnp.float32)
    products, local_state = lax.associative_scan(chain_step, (decay, inflow), axis=0)
    entering = carried_in(
        (products[-1], local_state[-1]),
        "sp",
        chain_step,
        (jnp.ones((rec_cols,), jnp.float32), jnp.zeros((rec_cols,), jnp.float32)),
    )
    state = local_state + products * entering[1][None, :]
    rec_out = (jax.nn.gelu(rec_gate.astype(jnp.float32)) * state).astype(jnp.bfloat16)
    nt_dims = (((1,), (1,)), ((), ()))
    return lax.psum_scatter(
        (
            lax.dot_general(conv_out, conv_full, nt_dims, preferred_element_type=jnp.float32)
            + lax.dot_general(
                rec_out, rec_full[:, :rec_cols], nt_dims, preferred_element_type=jnp.float32
            )
        ).astype(jnp.bfloat16),
        "tp",
        scatter_dimension=0,
        tiled=True,
    )


def solution(mesh):
    in_specs = (
        P(("sp", "tp"), None), P(), P("sp", "tp"), P("sp", "tp"), P("sp", "tp"), P("sp", "tp"),
        P(None, "tp"), P("tp"), P("tp"), P(None, "tp"), P("tp", None, None), P("tp", None, None),
        P("tp"), P("sp", "tp"), P("tp", "sp"), P("tp", "sp"),
    )
    return jax.shard_map(
        shards, mesh=mesh, in_specs=in_specs, out_specs=P(("sp", "tp"), None), check_vma=False
    )
```

```python
import jax
import jax.numpy as jnp
from jax import lax
from jax.experimental import pallas as pl
from jax.experimental.pallas import tpu as pltpu
from jax.sharding import PartitionSpec as P

MESH = pl.DeviceIdType.MESH
CONV_WIDTH = 1024
RATE_SCALE = 8.0
NZ, NY, NX, NC = 16, 4, 4, 2
HALF = NZ // 2


def rem(a, n):
    return lax.rem(a + 4 * n, n)


class Gather:
    def __init__(self, a, b, rows, sems, pos):
        self.a, self.b, self.rows = a, b, rows
        self.s, self.r = sems[: len(sems) // 2], sems[len(sems) // 2 :]
        self.z, self.y = pos
        self.sent = []

    def at(self, ref, z, y):
        rows = self.rows
        return ref.at[pl.ds(pl.multiple_of((rem(z, NZ) * NY + rem(y, NY)) * rows, rows), rows)]

    def copy(self, ref, chunk, kind, index, to):
        block = self.at(ref, *chunk)
        return pltpu.make_async_remote_copy(
            src_ref=block,
            dst_ref=block,
            send_sem=self.s[kind].at[index],
            recv_sem=self.r[kind].at[index],
            device_id={"sp": rem(to[0], NZ) * NY + rem(to[1], NY)},
            device_id_type=MESH,
        )

    def send(self, *args):
        self.copy(*args).start()
        self.sent.append(args)

    def arrived(self, ref, chunk, kind, index):
        self.copy(ref, chunk, kind, index, (self.z + 1, self.y)).wait_recv()

    def start(self):
        z, y, a, b = self.z, self.y, self.a, self.b
        self.send(b, (z, y), 3, 0, (z + 1, y))
        self.send(b, (z, y), 4, 0, (z - 1, y))
        self.send(a, (z, y), 0, 0, (z, y + 1))
        self.send(a, (z, y), 0, 2, (z, y + 3))
        self.send(a, (z, y), 0, 1, (z, y + 2))
        self.send(a, (z, y), 1, 0, (z + 1, y))
        self.send(a, (z, y), 2, 0, (z - 1, y))
        self.spread(0)

    def start_y(self):
        z, y, a = self.z, self.y, self.a
        for d in (1, 3, 2):
            self.arrived(a, (z, y - d), 0, d - 1)
            self.send(a, (z, y - d), 1, d, (z + 1, y))
            self.send(a, (z, y - d), 2, d, (z - 1, y))

    def spread(self, k):
        z, y = self.z, self.y
        self.send(self.b, (z - k, y), 5, 3 * k, (z, y + 1))
        self.send(self.b, (z - k, y), 5, 3 * k + 1, (z, y - 1))

    def along_z(self, s):
        z, y, a, b = self.z, self.y, self.a, self.b
        self.arrived(b, (z - s, y), 3, s - 1)
        if s < HALF:
            self.send(b, (z - s, y), 3, s, (z + 1, y))
            self.arrived(b, (z + s, y), 4, s - 1)
            if s < HALF - 1:
                self.send(b, (z + s, y), 4, s, (z - 1, y))
            self.spread(s)
            self.spread(NZ - s)
        else:
            self.spread(s)
        for d in (0, 1, 3, 2):
            self.arrived(a, (z - s, y - d), 1, 4 * (s - 1) + d)
            if s < HALF:
                self.send(a, (z - s, y - d), 1, 4 * s + d, (z + 1, y))
                self.arrived(a, (z + s, y - d), 2, 4 * (s - 1) + d)
                if s < HALF - 1:
                    self.send(a, (z + s, y - d), 2, 4 * s + d, (z - 1, y))

    def along_y(self, k):
        z, y = self.z, self.y
        turn = 1 - 2 * (k % 2)
        self.arrived(self.b, (z - k, y - 1), 5, 3 * k)
        self.arrived(self.b, (z - k, y + 1), 5, 3 * k + 1)
        self.send(self.b, (z - k, y - turn), 5, 3 * k + 2, (z, y + turn))

    def along_y_last(self, k):
        self.arrived(self.b, (self.z - k, self.y + 2), 5, 3 * k + 2)

    def finish(self):
        for args in self.sent:
            self.copy(*args).wait_send()

    @staticmethod
    def semaphores():
        counts = [3, 4 * HALF, 4 * HALF, HALF, HALF, 3 * NZ]
        return [pltpu.SemaphoreType.DMA((n,)) for n in counts + counts]


N_SEMS = 12


def groups_of(step):
    if step == 0:
        return [0]
    if step < HALF:
        return [step, NZ - step]
    return [step] if step == HALF else []


def expm1_negated(v):
    series = jnp.ones_like(v)
    for n in range(9, 1, -1):
        series = 1.0 + series * v * (1.0 / n)
    return jnp.where(v > -0.5, -v * series, 1.0 - jnp.exp(v))


def softplus_negated(b):
    e = jnp.exp(-jnp.abs(b))
    w = e / (2.0 + e)
    q = w * w
    series = jnp.full_like(w, 1.0 / 15.0)
    for n in (13, 11, 9, 7, 5, 3, 1):
        series = 1.0 / n + series * q
    return jnp.maximum(-b, 0.0) + 2.0 * w * series


NT_DIMS = (((1,), (1,)), ((), ()))
TN_DIMS = (((0,), (0,)), ((), ()))
SEGS = 8


def whole_kernel(
    tokens, gain, wc_own, wr_own, oc_own, or_own, taps, bias, cgain, staps, dmap, imap, base, jump, out, *scratch
):
    (nt, wc, wr, acc_c, acc_r, oc, orr, ext_c, ext_r, filt, md, mi, stats, dbuf, ibuf, gbuf, co, ro,
     seg_e, cy, cz, pc, ps, pr, s2, sp_buf, sm_buf, two, from_m, from_p) = scratch[:30]
    scratch = scratch[30:]
    sems_in, sems_out = scratch[:N_SEMS], scratch[N_SEMS : 2 * N_SEMS]
    (tok_s, tok_r, edge_s, edge_r, stat_s, stat_r, cy_s, cy_r, cz_s, cz_r, pr_s, pr_r, x_s, x_r) = scratch[2 * N_SEMS :]
    sp, tp = lax.axis_index("sp"), lax.axis_index("tp")
    z, y, x, c = sp // NY, sp % NY, tp // NC, tp % NC
    rows = wc_own.shape[0]
    n_tok, width = tokens.shape
    length = acc_c.shape[0]
    cw = acc_c.shape[1] // 2
    rw = acc_r.shape[1] // 2
    f32, bf16 = jnp.float32, jnp.bfloat16

    barrier = pltpu.get_barrier_semaphore()
    for dz, dy in ((1, 0), (-1, 0), (0, 1), (0, 2), (0, 3)):
        pl.semaphore_signal(
            barrier, inc=1, device_id={"sp": rem(z + dz, NZ) * NY + rem(y + dy, NY)}, device_id_type=MESH
        )
    for d in (1, -1):
        pl.semaphore_signal(barrier, inc=1, device_id={"sp": rem(sp + d, NZ * NY)}, device_id_type=MESH)
    for d in range(1, NX * NC):
        pl.semaphore_signal(barrier, inc=1, device_id={"tp": rem(tp + d, NX * NC)}, device_id_type=MESH)

    own = pl.ds(pl.multiple_of(sp * rows, rows), rows)
    wc[own] = wc_own[...]
    wr[own] = wr_own[...]
    oc[own] = oc_own[...]
    orr[own] = or_own[...]
    pl.semaphore_wait(barrier, 7 + NX * NC - 1)

    g_in = Gather(wc, wr, rows, sems_in, (z, y))
    g_out = Gather(oc, orr, rows, sems_out, (z, y))
    g_in.start()

    def tok_rows(xx, cc):
        return pl.ds(pl.multiple_of((rem(xx, NX) * NC + rem(cc, NC)) * n_tok, 16), n_tok)

    def tok_at(xx, cc, lanes=None):
        r = tok_rows(xx, cc)
        return nt.at[r] if lanes is None else nt.at[r, lanes]

    def tok_copy(block, index, xx, cc):
        return pltpu.make_async_remote_copy(
            src_ref=block, dst_ref=block, send_sem=tok_s.at[index], recv_sem=tok_r.at[index],
            device_id={"tp": rem(xx, NX) * NC + rem(cc, NC)}, device_id_type=MESH,
        )

    t_sent = []

    def tok_send(*args):
        tok_copy(*args).start()
        t_sent.append(args)

    lo, hi = pl.ds(0, width // 2), pl.ds(width // 2, width // 2)

    widened = tokens[...].astype(f32)
    inverse = lax.rsqrt(jnp.mean(widened * widened, axis=-1, keepdims=True) + 1e-06)
    tok_at(x, c)[...] = (widened * inverse * gain[...]).astype(bf16)
    tok_send(tok_at(x, c), 0, x + 1, c)
    tok_send(tok_at(x, c), 1, x - 1, c)
    tok_send(tok_at(x, c), 4, x, c + 1)
    g_in.start_y()
    acc_c[...] = jnp.zeros_like(acc_c)
    acc_r[...] = jnp.zeros_like(acc_r)
    cy[...] = jnp.zeros_like(cy)
    cz[...] = jnp.zeros_like(cz)
    head = dmap.shape[1]
    for m, given in ((md, dmap), (mi, imap)):
        m[...] = jnp.zeros_like(m)
        for h in range(dmap.shape[0]):
            m[h * head : (h + 1) * head, h * head : (h + 1) * head] = given[h]

    def tokens_forward():
        tok_copy(tok_at(x - 1, c), 0, x + 1, c).wait_recv()
        tok_send(tok_at(x - 1, c, lo), 2, x + 1, c)
        tok_send(tok_at(x - 1, c), 5, x, c + 1)
        tok_copy(tok_at(x + 1, c), 1, x + 1, c).wait_recv()
        tok_send(tok_at(x + 1, c, hi), 3, x - 1, c)
        tok_send(tok_at(x + 1, c), 6, x, c + 1)

    def tokens_last():
        tok_copy(tok_at(x + 2, c, lo), 2, x + 1, c).wait_recv()
        tok_send(tok_at(x + 2, c, lo), 7, x, c + 1)
        tok_copy(tok_at(x + 2, c, hi), 3, x + 1, c).wait_recv()
        tok_send(tok_at(x + 2, c, hi), 8, x, c + 1)
        tok_copy(tok_at(x, c + 1), 4, x + 1, c).wait_recv()
        tok_copy(tok_at(x - 1, c + 1), 5, x + 1, c).wait_recv()
        tok_copy(tok_at(x + 1, c + 1), 6, x + 1, c).wait_recv()
        tok_copy(tok_at(x + 2, c + 1, lo), 7, x + 1, c).wait_recv()
        tok_copy(tok_at(x + 2, c + 1, hi), 8, x + 1, c).wait_recv()

    def multiply(acc, w, first, count):
        def body(i, carry):
            cols = pl.ds(pl.multiple_of(rem(z - first - i, NZ) * (NY * rows), NY * rows), NY * rows)
            acc[...] += jnp.dot(nt[:, cols], w[cols, :], preferred_element_type=f32)
            return carry

        lax.fori_loop(0, count, body, 0)

    def multiply_runs(acc, w, steps):
        ks = sorted(k for s in steps for k in groups_of(s))
        runs = []
        for k in ks:
            if runs and runs[-1][0] + runs[-1][1] == k:
                runs[-1][1] += 1
            else:
                runs.append([k, 1])
        for first, count in runs:
            multiply(acc, w, first, count)

    go = 5
    for step in range(1, HALF + 3):
        if step == 2:
            g_out.start()
        if step <= HALF:
            g_in.along_z(step)
        if step == 3:
            g_out.start_y()
        if 2 < step:
            if step - 2 <= HALF:
                g_out.along_z(step - 2)
        for k in groups_of(step - 1):
            g_in.along_y(k)
        if step >= 2:
            for k in groups_of(step - 2):
                g_in.along_y_last(k)
        if step >= 4:
            for k in groups_of(step - 3):
                g_out.along_y(k)
        elif step == 3:
            g_out.along_y(0)
        if step == 3:
            tokens_forward()
        if step == go:
            tokens_last()
            multiply_runs(acc_c, wc, range(0, step + 1))
            multiply_runs(acc_r, wr, range(0, step - 1))
        elif step > go:
            multiply_runs(acc_c, wc, [step])
            multiply_runs(acc_r, wr, [step - 2])

    c_pad, r_pad = ext_c.shape[0] - length, ext_r.shape[0] - length
    projected = acc_r[...].astype(bf16).astype(f32)
    ext_r[r_pad:, :] = projected[:, :rw]
    gate = projected[:, rw:]
    conv_val = acc_c[:, :cw].astype(bf16).astype(f32)
    conv_gate = acc_c[:, cw:].astype(bf16).astype(f32)
    ext_c[c_pad:, :] = (conv_val * jax.nn.sigmoid(conv_gate)).astype(bf16).astype(f32)

    def edge_copy(ref, pad, index):
        return pltpu.make_async_remote_copy(
            src_ref=ref.at[pl.ds(length, pad)], dst_ref=ref.at[pl.ds(0, pad)],
            send_sem=edge_s.at[index], recv_sem=edge_r.at[index],
            device_id={"sp": rem(sp + 1, NZ * NY)}, device_id_type=MESH,
        )

    edges = [edge_copy(ext_r, r_pad, 0), edge_copy(ext_c, c_pad, 1)]
    for e in edges:
        e.start()
    for k in groups_of(HALF):
        g_out.along_y(k)
    gbuf[...] = 0.5 * gate * (1.0 + jnp.tanh(0.7978845608028654 * (gate + 0.044715 * gate * gate * gate)))

    n_taps = taps.shape[0]
    wide = taps[...].astype(f32)
    tap_rows = 32

    def filter_rows(first):
        total = jnp.broadcast_to(bias[...], (tap_rows, cw))
        for k in range(n_taps):
            at = first + c_pad - (n_taps - 1) + k
            total = total + wide[k : k + 1, :] * ext_c[at : at + tap_rows, :]
        filt[first : first + tap_rows, :] = total

    for i in range(1, length // tap_rows):
        filter_rows(i * tap_rows)
    for e in edges:
        e.wait_recv()
    has = sp > 0
    ext_r[:r_pad, :] = jnp.where(has, ext_r[:r_pad, :], 0.0)
    ext_c[:c_pad, :] = jnp.where(has, ext_c[:c_pad, :], 0.0)
    filter_rows(0)

    filtered = filt[...]
    row_id = lax.broadcasted_iota(jnp.int32, (8, cw), 0)
    first_half = jnp.where(row_id < 4, 1.0, 0.0)
    exact = lax.Precision.HIGHEST
    stats[tp] = lax.dot_general(
        first_half, filtered, NT_DIMS, precision=exact, preferred_element_type=f32
    ) + lax.dot_general(
        1.0 - first_half, filtered * filtered, NT_DIMS, precision=exact, preferred_element_type=f32
    )

    def stat_copy(d):
        return pltpu.make_async_remote_copy(
            src_ref=stats.at[tp], dst_ref=stats.at[tp], send_sem=stat_s.at[d - 1], recv_sem=stat_r.at[d - 1],
            device_id={"tp": rem(tp + d, NX * NC)}, device_id_type=MESH,
        )

    def stat_arrival(d):
        slot = stats.at[rem(tp - d, NX * NC)]
        return pltpu.make_async_remote_copy(
            src_ref=slot, dst_ref=slot, send_sem=stat_s.at[d - 1], recv_sem=stat_r.at[d - 1],
            device_id={"tp": rem(tp + d, NX * NC)}, device_id_type=MESH,
        )

    for d in range(1, NX * NC):
        stat_copy(d).start()

    n_short = staps.shape[0]
    short = staps[...].astype(f32)
    smoothed = jnp.zeros((length, rw), f32)
    for k in range(n_short):
        at = r_pad - (n_short - 1) + k
        smoothed = smoothed + short[k : k + 1, :] * ext_r[at : at + length, :]
    rounded = smoothed.astype(bf16)
    retain = jax.nn.sigmoid(jnp.dot(rounded, md[...], preferred_element_type=f32))
    admit = jax.nn.sigmoid(jnp.dot(rounded, mi[...], preferred_element_type=f32))
    log_decay = (-RATE_SCALE * softplus_negated(base[...])) * retain + jump[...]
    decay = jnp.exp(log_decay)
    inflow = jnp.sqrt(expm1_negated(2.0 * log_decay)) * admit * rounded.astype(f32)
    tile = 128
    n_tiles = dbuf.shape[0]
    for n in range(n_tiles):
        used = min(tile, rw - n * tile)
        dbuf[n, :, :used] = decay[:, n * tile : n * tile + used]
        ibuf[n, :, :used] = inflow[:, n * tile : n * tile + used]
    seg = length // SEGS

    def scan_step(j, carry):
        new = []
        for n, (p, s) in enumerate(carry):
            at = (n, pl.ds(j, SEGS, stride=seg), slice(None))
            d, i = dbuf[at], ibuf[at]
            p, s = d * p, d * s + i
            dbuf[at] = p
            ibuf[at] = s
            new.append((p, s))
        return tuple(new)

    start = tuple((jnp.ones((SEGS, tile), f32), jnp.zeros((SEGS, tile), f32)) for _ in range(n_tiles))
    ends = lax.fori_loop(0, seg, scan_step, start)
    p_all = jnp.concatenate([e[0] for e in ends], axis=1)
    s_all = jnp.concatenate([e[1] for e in ends], axis=1)
    half = cy.shape[2] // 2
    p_run, s_run = jnp.ones((1, half), f32), jnp.zeros((1, half), f32)
    before = []
    for g in range(SEGS):
        before.append((p_run, s_run))
        p_g, s_g = p_all[g : g + 1, :], s_all[g : g + 1, :]
        p_run, s_run = p_run * p_g, p_g * s_run + s_g

    def carry_copy(buf, slot, send, recv, d, to):
        return pltpu.make_async_remote_copy(
            src_ref=buf.at[slot], dst_ref=buf.at[slot], send_sem=send.at[d - 1], recv_sem=recv.at[d - 1],
            device_id={"sp": rem(to[0], NZ) * NY + rem(to[1], NY)}, device_id_type=MESH,
        )

    cy[y, :, :half] = p_run
    cy[y, :, half:] = s_run
    for d in range(1, NY):
        carry_copy(cy, y, cy_s, cy_r, d, (z, y + d)).start()

    for d in range(1, NX * NC):
        stat_arrival(d).wait_recv()
    totals = stats[0]
    for n in range(1, NX * NC):
        totals = totals + stats[n]
    scale = 1.0 / CONV_WIDTH
    row_id = lax.broadcasted_iota(jnp.int32, (8, cw), 0)
    mean = lax.dot_general(
        totals * scale, jnp.where(row_id == 0, 1.0, 0.0), TN_DIMS, precision=exact, preferred_element_type=f32
    )
    square = lax.dot_general(
        totals * scale, jnp.where(row_id == 4, 1.0, 0.0), TN_DIMS, precision=exact, preferred_element_type=f32
    )

    for d in range(1, NY):
        carry_copy(cy, rem(y - d, NY), cy_s, cy_r, d, (z, y + d)).wait_recv()
    p_run, s_run = jnp.ones((1, half), f32), jnp.zeros((1, half), f32)
    p_mine, s_mine = p_run, s_run
    for n in range(NY):
        p_mine = jnp.where(y == n, p_run, p_mine)
        s_mine = jnp.where(y == n, s_run, s_mine)
        p_n, s_n = cy[n, :, :half], cy[n, :, half:]
        p_run, s_run = p_run * p_n, p_n * s_run + s_n
    cz[z, :, :half] = p_run
    cz[z, :, half:] = s_run
    for d in range(1, NZ):
        carry_copy(cz, z, cz_s, cz_r, d, (z + d, y)).start()

    spread = jnp.maximum(square - mean * mean, 0.0)
    scaled = (filt[...] - mean) * lax.rsqrt(spread + 1e-05) * cgain[...]
    co[...] = (scaled * jax.nn.sigmoid(scaled)).astype(bf16)
    for k in range(NZ):
        g_out.along_y_last(k)
    block = 512

    def conv_part(j, carry):
        cols = pl.ds(pl.multiple_of(j * block, block), block)
        pc[:, cols] = lax.dot_general(co[...], oc[cols, :], NT_DIMS, preferred_element_type=f32)
        return carry

    lax.fori_loop(0, width // block, conv_part, 0)

    for d in range(1, NZ):
        carry_copy(cz, rem(z - d, NZ), cz_s, cz_r, d, (z + d, y)).wait_recv()
    entering = jnp.zeros((1, half), f32)
    for n in range(NZ):
        entering = jnp.where(n < z, cz[n, :, :half] * entering + cz[n, :, half:], entering)
    entering = p_mine * entering + s_mine
    for g, (p_g, s_g) in enumerate(before):
        part = slice(g * seg, (g + 1) * seg)
        at_start = p_g * entering + s_g
        for n in range(n_tiles):
            used = min(tile, rw - n * tile)
            lanes = slice(n * tile, n * tile + used)
            state = ibuf[n, part, :used] + dbuf[n, part, :used] * at_start[:, lanes]
            ro[part, lanes] = (gbuf[part, lanes] * state).astype(bf16)

    def chip_rows(xx, cc):
        return pl.ds(pl.multiple_of((rem(xx, NX) * NC + rem(cc, NC)) * n_tok, n_tok), n_tok)

    def rec_part(j, carry):
        cols = pl.ds(pl.multiple_of(j * block, block), block)
        pc[:, cols] += lax.dot_general(ro[...], orr[cols, :rw], NT_DIMS, preferred_element_type=f32)
        for d in range(NX):
            ps[d, :, cols] = pc[chip_rows(x + d, c + 1), cols].astype(bf16)
        return carry

    def pair_copy(d, side):
        lanes = (lo, hi)[side]
        return pltpu.make_async_remote_copy(
            src_ref=ps.at[d, :, lanes], dst_ref=pr.at[d, :, lanes],
            send_sem=pr_s.at[2 * d + side], recv_sem=pr_r.at[2 * d + side],
            device_id={"tp": x * NC + rem(c + 1, NC)}, device_id_type=MESH,
        )

    for side in range(2):
        n_blocks = width // block // 2
        lax.fori_loop(side * n_blocks, (side + 1) * n_blocks, rec_part, 0)
        for d in (2, 1, 3, 0):
            pair_copy(d, side).start()

    def x_copy(src, dst, index, xx):
        return pltpu.make_async_remote_copy(
            src_ref=src, dst_ref=dst, send_sem=x_s.at[index], recv_sem=x_r.at[index],
            device_id={"tp": rem(xx, NX) * NC + c}, device_id_type=MESH,
        )

    halves = (slice(0, width // 2), slice(width // 2, width))

    def chip_sum(d, side):
        h = halves[side]
        return pc[chip_rows(x + d, c), h] + pr[d, :, h].astype(f32)

    copies = [
        x_copy(s2.at[:, lo], two.at[:, lo], 0, x + 1),
        x_copy(s2.at[:, hi], two.at[:, hi], 1, x - 1),
        x_copy(sp_buf.at[:, hi], from_m.at[:, hi], 2, x + 1),
        x_copy(sm_buf.at[:, lo], from_p.at[:, lo], 3, x - 1),
        x_copy(sp_buf.at[:, lo], from_m.at[:, lo], 4, x + 1),
        x_copy(sm_buf.at[:, hi], from_p.at[:, hi], 5, x - 1),
    ]
    for side in range(2):
        pair_copy(2, side).wait_recv()
        s2[:, halves[side]] = chip_sum(2, side).astype(bf16)
        copies[side].start()
    pair_copy(3, 0).wait_recv()
    sm_buf[:, halves[0]] = chip_sum(3, 0).astype(bf16)
    copies[3].start()
    pair_copy(1, 1).wait_recv()
    sp_buf[:, halves[1]] = chip_sum(1, 1).astype(bf16)
    copies[2].start()
    pair_copy(1, 0).wait_recv()
    copies[0].wait_recv()
    sp_buf[:, halves[0]] = (chip_sum(1, 0) + two[:, halves[0]].astype(f32)).astype(bf16)
    copies[4].start()
    pair_copy(3, 1).wait_recv()
    copies[1].wait_recv()
    sm_buf[:, halves[1]] = (chip_sum(3, 1) + two[:, halves[1]].astype(f32)).astype(bf16)
    copies[5].start()
    mine = chip_rows(x, c)
    for side in range(2):
        pair_copy(0, side).wait_recv()
        pc[mine, halves[side]] = chip_sum(0, side)
    for n in range(2, 6):
        copies[n].wait_recv()
    out[...] = (pc[mine, :] + (from_m[...].astype(f32) + from_p[...].astype(f32))).astype(bf16)

    g_in.finish()
    g_out.finish()
    for args in t_sent:
        tok_copy(*args).wait_send()
    for e in edges:
        e.wait_send()
    for d in range(1, NX * NC):
        stat_copy(d).wait_send()
    for d in range(1, NY):
        carry_copy(cy, y, cy_s, cy_r, d, (z, y + d)).wait_send()
    for d in range(1, NZ):
        carry_copy(cz, z, cz_s, cz_r, d, (z + d, y)).wait_send()
    for side in range(2):
        for d in range(NX):
            pair_copy(d, side).wait_send()
    for n in copies:
        n.wait_send()


def shards(
    tokens, norm_gain, conv_val_w, conv_gate_w, rec_gate_w, rec_in_w, conv_taps, conv_bias, conv_gain,
    short_taps, decay_map, input_map, decay_base, decay_jump, out_conv_w, out_rec_w,
):
    cw, rw = conv_val_w.shape[1], rec_in_w.shape[1]
    n_tok, width = tokens.shape
    length = n_tok * NX * NC
    wide = rw + -rw % 128
    f32, bf16 = jnp.float32, jnp.bfloat16
    vmem = pl.BlockSpec(memory_space=pltpu.VMEM)
    V, S = pltpu.VMEM, pltpu.SemaphoreType.DMA
    return pl.pallas_call(
        whole_kernel,
        out_shape=jax.ShapeDtypeStruct((n_tok, width), bf16),
        in_specs=[vmem] * 14,
        out_specs=vmem,
        scratch_shapes=[
            V((length, width), bf16),
            V((width, 2 * cw), bf16),
            V((width, 2 * rw), bf16),
            V((length, 2 * cw), f32),
            V((length, 2 * rw), f32),
            V((width, cw), bf16),
            V((width, wide), bf16),
            V((length + 32, cw), f32),
            V((length + 8, rw), f32),
            V((length, cw), f32),
            V((rw, rw), bf16),
            V((rw, rw), bf16),
            V((NX * NC, 8, length), f32),
            V((wide // 128, length, 128), f32),
            V((wide // 128, length, 128), f32),
            V((length, rw), f32),
            V((length, cw), bf16),
            V((length, rw), bf16),
            V((8, 128), f32),
            V((NY, 1, 2 * wide), f32),
            V((NZ, 1, 2 * wide), f32),
            V((length, width), f32),
            V((NX, n_tok, width), bf16),
            V((NX, n_tok, width), bf16),
            V((n_tok, width), bf16),
            V((n_tok, width), bf16),
            V((n_tok, width), bf16),
            V((n_tok, width), bf16),
            V((n_tok, width), bf16),
            V((n_tok, width), bf16),
            *Gather.semaphores(),
            *Gather.semaphores(),
            S((9,)), S((9,)), S((2,)), S((2,)), S((7,)), S((7,)), S((3,)), S((3,)),
            S((NZ - 1,)), S((NZ - 1,)), S((2 * NX,)), S((2 * NX,)), S((6,)), S((6,)),
        ],
        compiler_params=pltpu.CompilerParams(
            collective_id=0, has_side_effects=True, vmem_limit_bytes=60 * 1024 * 1024
        ),
    )(
        tokens,
        norm_gain[None, :],
        jnp.concatenate([conv_val_w, conv_gate_w], axis=1),
        jnp.concatenate([rec_in_w, rec_gate_w], axis=1),
        out_conv_w.T,
        jnp.pad(out_rec_w.T, ((0, 0), (0, wide - rw))),
        conv_taps,
        conv_bias[None, :],
        conv_gain[None, :],
        short_taps,
        decay_map,
        input_map,
        decay_base[None, :],
        decay_jump,
    )


def solution(mesh):
    in_specs = (
        P(("sp", "tp"), None), P(), P("sp", "tp"), P("sp", "tp"), P("sp", "tp"), P("sp", "tp"),
        P(None, "tp"), P("tp"), P("tp"), P(None, "tp"), P("tp", None, None), P("tp", None, None),
        P("tp"), P("sp", "tp"), P("tp", "sp"), P("tp", "sp"),
    )
    return jax.shard_map(
        shards, mesh=mesh, in_specs=in_specs, out_specs=P(("sp", "tp"), None), check_vma=False
    )
```

```python
import jax
import jax.numpy as jnp
from jax import lax
from jax.experimental import pallas as pl
from jax.experimental.pallas import tpu as pltpu
from jax.sharding import PartitionSpec as P

MESH = pl.DeviceIdType.MESH
CONV_WIDTH = 1024
RATE_SCALE = 8.0
NZ, NY, NX, NC = 16, 4, 4, 2
HALF = NZ // 2


def rem(a, n):
    return lax.rem(a + 4 * n, n)


class Gather:
    def __init__(self, a, b, rows, sems, pos):
        self.a, self.b = a, b
        self.rows = {id(a): rows[0], id(b): rows[1]}
        self.s, self.r = sems[: len(sems) // 2], sems[len(sems) // 2 :]
        self.z, self.y = pos
        self.sent = []

    def at(self, ref, z, y):
        rows = self.rows[id(ref)]
        return ref.at[pl.ds(pl.multiple_of((rem(z, NZ) * NY + rem(y, NY)) * rows, rows), rows)]

    def copy(self, ref, chunk, kind, index, to):
        block = self.at(ref, *chunk)
        return pltpu.make_async_remote_copy(
            src_ref=block,
            dst_ref=block,
            send_sem=self.s[kind].at[index],
            recv_sem=self.r[kind].at[index],
            device_id={"sp": rem(to[0], NZ) * NY + rem(to[1], NY)},
            device_id_type=MESH,
        )

    def send(self, *args):
        self.copy(*args).start()
        self.sent.append(args)

    def arrived(self, ref, chunk, kind, index):
        self.copy(ref, chunk, kind, index, (self.z + 1, self.y)).wait_recv()

    def start_y(self):
        z, y, a = self.z, self.y, self.a
        for d in (1, 3, 2):
            self.send(a, (z, y), 0, d - 1, (z, y + d))

    def start_z(self):
        z, y = self.z, self.y
        for ref, up in ((self.b, 3), (self.a, 1)):
            self.send(ref, (z, y), up, 0, (z + 1, y))
            self.send(ref, (z, y), up + 1, 0, (z - 1, y))

    def from_y(self):
        z, y, a = self.z, self.y, self.a
        for d in (1, 3, 2):
            self.arrived(a, (z, y - d), 0, d - 1)
            self.send(a, (z, y - d), 1, d, (z + 1, y))
            self.send(a, (z, y - d), 2, d, (z - 1, y))

    def spread(self, k):
        z, y = self.z, self.y
        self.send(self.b, (z - k, y), 5, 3 * k, (z, y + 1))
        self.send(self.b, (z - k, y), 5, 3 * k + 1, (z, y - 1))
        if k == HALF:
            self.send(self.b, (z - k, y), 5, 3 * k + 2, (z, y + 2))

    def along_z(self, s, between=lambda: None):
        z, y, a, b = self.z, self.y, self.a, self.b
        last, next_last = s == HALF, s + 1 == HALF
        self.arrived(b, (z - s, y), 3, s - 1)
        if not last:
            self.send(b, (z - s, y), 3, s, (z + 1, y))
            self.arrived(b, (z + s, y), 4, s - 1)
            if not next_last:
                self.send(b, (z + s, y), 4, s, (z - 1, y))
            self.spread(s)
            self.spread(NZ - s)
        else:
            self.spread(s)
        for d in (0, 1, 3, 2):
            if not last or d == 0:
                self.arrived(a, (z - s, y - d), 1, 4 * (s - 1) + d)
            if not last and not (next_last and d > 0):
                self.send(a, (z - s, y - d), 1, 4 * s + d, (z + 1, y))
            if not last or d > 0:
                self.arrived(a, (z + s, y - d), 2, 4 * (s - 1) + d)
            if not last and not (next_last and d == 0):
                self.send(a, (z + s, y - d), 2, 4 * s + d, (z - 1, y))
            between()

    def along_y(self, k):
        z, y = self.z, self.y
        turn = 1 - 2 * (k % 2)
        self.arrived(self.b, (z - k, y - 1), 5, 3 * k)
        self.arrived(self.b, (z - k, y + 1), 5, 3 * k + 1)
        if k != HALF:
            self.send(self.b, (z - k, y - turn), 5, 3 * k + 2, (z, y + turn))

    def along_y_last(self, k):
        self.arrived(self.b, (self.z - k, self.y + 2), 5, 3 * k + 2)

    def finish(self):
        for args in self.sent:
            self.copy(*args).wait_send()

    @staticmethod
    def semaphores():
        counts = [3, 4 * HALF, 4 * HALF, HALF, HALF, 3 * NZ]
        return [pltpu.SemaphoreType.DMA((n,)) for n in counts + counts]


N_SEMS = 12


def groups_of(step):
    if step == 0:
        return [0]
    if step < HALF:
        return [step, NZ - step]
    return [step] if step == HALF else []


def expm1_negated(v):
    series = jnp.ones_like(v)
    for n in range(9, 1, -1):
        series = 1.0 + series * v * (1.0 / n)
    return jnp.where(v > -0.5, -v * series, 1.0 - jnp.exp(v))


def softplus_negated(b):
    e = jnp.exp(-jnp.abs(b))
    w = e / (2.0 + e)
    q = w * w
    series = jnp.full_like(w, 1.0 / 15.0)
    for n in (13, 11, 9, 7, 5, 3, 1):
        series = 1.0 / n + series * q
    return jnp.maximum(-b, 0.0) + 2.0 * w * series


NT_DIMS = (((1,), (1,)), ((), ()))
TN_DIMS = (((0,), (0,)), ((), ()))
SEGS = 8


def whole_kernel(
    tokens, gain, wv_own, wg_own, ri_own, rg_own, oc_own, or_own, taps, bias, cgain, staps, dmap, imap, base, jump_t, out, *scratch
):
    (nt, wa, wb, acc_a, acc_b, oc, packed, orr, ext_c, ext_r, filt, md, mi, stats, dbuf, ibuf, gbuf, co, ro,
     jump, cy, cz, pc, ps, pr, s2, sp_buf, sm_buf, two, from_m, from_p) = scratch[:31]
    scratch = scratch[31:]
    sems_in, sems_out = scratch[:N_SEMS], scratch[N_SEMS : 2 * N_SEMS]
    (tok_s, tok_r, edge_s, edge_r, stat_s, stat_r, cy_s, cy_r, cz_s, cz_r, pr_s, pr_r, x_s, x_r) = scratch[2 * N_SEMS :]
    sp, tp = lax.axis_index("sp"), lax.axis_index("tp")
    z, y, x, c = sp // NY, sp % NY, tp // NC, tp % NC
    rows = wv_own.shape[0]
    n_tok, width = tokens.shape
    length = acc_a.shape[0]
    cw, rw = wv_own.shape[1], ri_own.shape[1]
    f32, bf16 = jnp.float32, jnp.bfloat16

    barrier = pltpu.get_barrier_semaphore()
    for dz, dy in ((1, 0), (-1, 0), (0, 1), (0, 2), (0, 3)):
        pl.semaphore_signal(
            barrier, inc=1, device_id={"sp": rem(z + dz, NZ) * NY + rem(y + dy, NY)}, device_id_type=MESH
        )
    for d in (1, -1):
        pl.semaphore_signal(barrier, inc=1, device_id={"sp": rem(sp + d, NZ * NY)}, device_id_type=MESH)
    for d in range(1, NX * NC):
        pl.semaphore_signal(barrier, inc=1, device_id={"tp": rem(tp + d, NX * NC)}, device_id_type=MESH)

    own = pl.ds(pl.multiple_of(sp * rows, rows), rows)
    extra = wa.shape[1] - rw
    wa[own, :] = jnp.concatenate([ri_own[...], rg_own[:, :extra]], axis=1)
    wb[own, :cw] = wv_own[...]
    wb[own, cw : 2 * cw] = wg_own[...]
    wb[own, 2 * cw :] = rg_own[:, extra:]
    oc[own] = oc_own[...]
    p_rows, h_rows = rows + rows // 2, rows // 2
    p_at = pl.multiple_of(sp * p_rows, h_rows)
    packed[pl.ds(p_at, rows)] = or_own[:, :128]
    packed[pl.ds(p_at + rows, h_rows)] = jnp.concatenate([or_own[:h_rows, 128:], or_own[h_rows:, 128:]], axis=1)

    def unpack(k):
        for n in range(NY):
            chunk = rem(z - k, NZ) * NY + n
            src = pl.multiple_of(chunk * p_rows, h_rows)
            dst = pl.multiple_of(chunk * rows, rows)
            orr[pl.ds(dst, rows), :128] = packed[pl.ds(src, rows)]
            pair = packed[pl.ds(src + rows, h_rows)]
            orr[pl.ds(dst, h_rows), 128:rw] = pair[:, : rw - 128]
            orr[pl.ds(dst + h_rows, h_rows), 128:rw] = pair[:, rw - 128 :]

    pl.semaphore_wait(barrier, 7 + NX * NC - 1)

    g_in = Gather(wa, wb, (rows, rows), sems_in, (z, y))
    g_out = Gather(oc, packed, (rows, rows + rows // 2), sems_out, (z, y))
    g_in.start_z()
    g_in.start_y()
    g_in.spread(0)
    g_out.start_z()

    def tok_rows(xx, cc):
        return pl.ds(pl.multiple_of((rem(xx, NX) * NC + rem(cc, NC)) * n_tok, 16), n_tok)

    def tok_at(xx, cc, lanes=None):
        r = tok_rows(xx, cc)
        return nt.at[r] if lanes is None else nt.at[r, lanes]

    def tok_copy(block, index, xx, cc):
        return pltpu.make_async_remote_copy(
            src_ref=block, dst_ref=block, send_sem=tok_s.at[index], recv_sem=tok_r.at[index],
            device_id={"tp": rem(xx, NX) * NC + rem(cc, NC)}, device_id_type=MESH,
        )

    t_sent = []

    def tok_send(*args):
        tok_copy(*args).start()
        t_sent.append(args)

    lo, hi = pl.ds(0, width // 2), pl.ds(width // 2, width // 2)

    widened = tokens[...].astype(f32)
    inverse = lax.rsqrt(jnp.mean(widened * widened, axis=-1, keepdims=True) + 1e-06)
    tok_at(x, c)[...] = (widened * inverse * gain[...]).astype(bf16)
    tok_send(tok_at(x, c), 0, x + 1, c)
    tok_send(tok_at(x, c), 1, x - 1, c)
    tok_send(tok_at(x, c), 4, x, c + 1)
    g_in.from_y()
    g_out.start_y()
    acc_a[...] = jnp.zeros_like(acc_a)
    acc_b[...] = jnp.zeros_like(acc_b)
    cy[...] = jnp.zeros_like(cy)
    cz[...] = jnp.zeros_like(cz)
    head = dmap.shape[1]
    for m, given in ((md, dmap), (mi, imap)):
        m[...] = jnp.zeros_like(m)
        for h in range(dmap.shape[0]):
            m[h * head : (h + 1) * head, h * head : (h + 1) * head] = given[h]
    jump[...] = jnp.transpose(jump_t[...])

    def tokens_forward():
        tok_copy(tok_at(x - 1, c), 0, x + 1, c).wait_recv()
        tok_send(tok_at(x - 1, c, lo), 2, x + 1, c)
        tok_send(tok_at(x - 1, c), 5, x, c + 1)
        tok_copy(tok_at(x + 1, c), 1, x + 1, c).wait_recv()
        tok_send(tok_at(x + 1, c, hi), 3, x - 1, c)
        tok_send(tok_at(x + 1, c), 6, x, c + 1)

    def tokens_relay():
        tok_copy(tok_at(x + 2, c, lo), 2, x + 1, c).wait_recv()
        tok_send(tok_at(x + 2, c, lo), 7, x, c + 1)
        tok_copy(tok_at(x + 2, c, hi), 3, x + 1, c).wait_recv()
        tok_send(tok_at(x + 2, c, hi), 8, x, c + 1)

    def tokens_last():
        tok_copy(tok_at(x, c + 1), 4, x + 1, c).wait_recv()
        tok_copy(tok_at(x - 1, c + 1), 5, x + 1, c).wait_recv()
        tok_copy(tok_at(x + 1, c + 1), 6, x + 1, c).wait_recv()
        tok_copy(tok_at(x + 2, c + 1, lo), 7, x + 1, c).wait_recv()
        tok_copy(tok_at(x + 2, c + 1, hi), 8, x + 1, c).wait_recv()

    def multiply(acc, w, first, last):
        def body(j, carry):
            s = (j + 1) // 2
            zz = rem(z + jnp.where(j % 2 == 1, -s, s), NZ)
            cols = pl.ds(pl.multiple_of(zz * (NY * rows), NY * rows), NY * rows)
            acc[...] += jnp.dot(nt[:, cols], w[cols, :], preferred_element_type=f32)
            return carry

        lax.fori_loop(first, last, body, 0)

    a_part = lambda first, last: (lambda: multiply(acc_a, wa, first, last))
    b_part = lambda first, last: (lambda: multiply(acc_b, wb, first, last))
    work = {
        6: [a_part(0, 2), a_part(2, 4), a_part(4, 6), a_part(6, 8)],
        7: [a_part(8, 10), a_part(10, 12), b_part(0, 2), b_part(2, 4)],
        8: [b_part(4, 6), b_part(6, 8), b_part(8, 10), a_part(12, 15)],
    }

    def out_step(s):
        if s == 0:
            g_out.spread(0)
            g_out.from_y()
        elif s <= HALF:
            g_out.along_z(s)
        if s >= 1:
            for k in groups_of(s - 1):
                g_out.along_y(k)
        if s >= 2:
            for k in groups_of(s - 2):
                g_out.along_y_last(k)
                unpack(k)

    lag = 4

    def at_step(step):
        todo = list(work.get(step, []))
        g_in.along_z(step, lambda: todo and todo.pop(0)())
        if step == HALF:
            a_part(NZ - 1, NZ)()
            start_recurrence()
        for k in groups_of(step - 1):
            g_in.along_y(k)
        if step >= lag:
            out_step(step - lag)
        if step >= 2:
            for k in groups_of(step - 2):
                g_in.along_y_last(k)
        if step == 2:
            tokens_forward()
        if step == 4:
            tokens_relay()
        if step == 5:
            tokens_last()

    c_pad, r_pad = ext_c.shape[0] - length, ext_r.shape[0] - length

    def edge_copy(ref, pad, index):
        return pltpu.make_async_remote_copy(
            src_ref=ref.at[pl.ds(length, pad)], dst_ref=ref.at[pl.ds(0, pad)],
            send_sem=edge_s.at[index], recv_sem=edge_r.at[index],
            device_id={"sp": rem(sp + 1, NZ * NY)}, device_id_type=MESH,
        )

    edges = [edge_copy(ext_r, r_pad, 0), edge_copy(ext_c, c_pad, 1)]

    def take_edge(index, ref, pad):
        edges[index].wait_recv()
        ref[:pad, :] = jnp.where(sp > 0, ref[:pad, :], 0.0)

    def start_recurrence():
        ext_r[r_pad:, :] = acc_a[:, :rw].astype(bf16).astype(f32)
        edges[0].start()

    for step in range(1, HALF + 1):
        at_step(step)

    n_short = staps.shape[0]
    short = staps[...].astype(f32)
    rate = -RATE_SCALE * softplus_negated(base[...])
    tile = 128
    n_tiles = dbuf.shape[0]

    def gates(first, count):
        smoothed = jnp.zeros((count, rw), f32)
        for k in range(n_short):
            at = r_pad - (n_short - 1) + k + first
            smoothed = smoothed + short[k : k + 1, :] * ext_r[at : at + count, :]
        rounded = smoothed.astype(bf16)
        retain = jax.nn.sigmoid(jnp.dot(rounded, md[...], preferred_element_type=f32))
        admit = jax.nn.sigmoid(jnp.dot(rounded, mi[...], preferred_element_type=f32))
        log_decay = rate * retain + jump[first : first + count, :]
        decay = jnp.exp(log_decay)
        inflow = jnp.sqrt(expm1_negated(2.0 * log_decay)) * admit * rounded.astype(f32)
        for n in range(n_tiles):
            used = min(tile, rw - n * tile)
            dbuf[n, first : first + count, :used] = decay[:, n * tile : n * tile + used]
            ibuf[n, first : first + count, :used] = inflow[:, n * tile : n * tile + used]

    early = 16
    gates(early, length - early)
    b_part(10, 13)()
    out_step(HALF + 1 - lag)
    take_edge(0, ext_r, r_pad)
    gates(0, early)
    seg = length // SEGS

    def scan_step(j, carry):
        new = []
        for n, (p, s) in enumerate(carry):
            at = (n, pl.ds(j, SEGS, stride=seg), slice(None))
            d, i = dbuf[at], ibuf[at]
            p, s = d * p, d * s + i
            dbuf[at] = p
            ibuf[at] = s
            new.append((p, s))
        return tuple(new)

    start = tuple((jnp.ones((SEGS, tile), f32), jnp.zeros((SEGS, tile), f32)) for _ in range(n_tiles))
    ends = lax.fori_loop(0, seg, scan_step, start)
    p_all = jnp.concatenate([e[0] for e in ends], axis=1)
    s_all = jnp.concatenate([e[1] for e in ends], axis=1)
    half = cy.shape[2] // 2
    p_run, s_run = jnp.ones((1, half), f32), jnp.zeros((1, half), f32)
    before = []
    for g in range(SEGS):
        before.append((p_run, s_run))
        p_g, s_g = p_all[g : g + 1, :], s_all[g : g + 1, :]
        p_run, s_run = p_run * p_g, p_g * s_run + s_g

    def carry_copy(buf, slot, send, recv, d, to):
        return pltpu.make_async_remote_copy(
            src_ref=buf.at[slot], dst_ref=buf.at[slot], send_sem=send.at[d - 1], recv_sem=recv.at[d - 1],
            device_id={"sp": rem(to[0], NZ) * NY + rem(to[1], NY)}, device_id_type=MESH,
        )

    cy[y, :, :half] = p_run
    cy[y, :, half:] = s_run
    for d in range(1, NY):
        carry_copy(cy, y, cy_s, cy_r, d, (z, y + d)).start()
    for k in groups_of(HALF):
        g_in.along_y(k)
    for k in groups_of(HALF - 1) + groups_of(HALF):
        g_in.along_y_last(k)
    b_part(13, NZ)()
    conv_val = acc_b[:, :cw].astype(bf16).astype(f32)
    conv_gate = acc_b[:, cw : 2 * cw].astype(bf16).astype(f32)
    ext_c[c_pad:, :] = (conv_val * jax.nn.sigmoid(conv_gate)).astype(bf16).astype(f32)
    edges[1].start()
    gate = jnp.concatenate([acc_a[:, rw:], acc_b[:, 2 * cw :]], axis=1).astype(bf16).astype(f32)
    gbuf[...] = 0.5 * gate * (1.0 + jnp.tanh(0.7978845608028654 * (gate + 0.044715 * gate * gate * gate)))
    out_step(HALF + 2 - lag)
    n_taps = taps.shape[0]
    wide = taps[...].astype(f32)
    tap_rows = 32

    def filter_rows(first):
        total = jnp.broadcast_to(bias[...], (tap_rows, cw))
        for k in range(n_taps):
            at = first + c_pad - (n_taps - 1) + k
            total = total + wide[k : k + 1, :] * ext_c[at : at + tap_rows, :]
        filt[first : first + tap_rows, :] = total

    for i in range(1, length // tap_rows):
        filter_rows(i * tap_rows)
    for d in range(1, NY):
        carry_copy(cy, rem(y - d, NY), cy_s, cy_r, d, (z, y + d)).wait_recv()
    p_run, s_run = jnp.ones((1, half), f32), jnp.zeros((1, half), f32)
    p_mine, s_mine = p_run, s_run
    for n in range(NY):
        p_mine = jnp.where(y == n, p_run, p_mine)
        s_mine = jnp.where(y == n, s_run, s_mine)
        p_n, s_n = cy[n, :, :half], cy[n, :, half:]
        p_run, s_run = p_run * p_n, p_n * s_run + s_n
    cz[z, :, :half] = p_run
    cz[z, :, half:] = s_run
    for d in range(1, NZ):
        carry_copy(cz, z, cz_s, cz_r, d, (z + d, y)).start()
    take_edge(1, ext_c, c_pad)
    filter_rows(0)
    filtered = filt[...]
    row_id = lax.broadcasted_iota(jnp.int32, (8, cw), 0)
    first_half = jnp.where(row_id < 4, 1.0, 0.0)
    exact = lax.Precision.HIGHEST
    stats[tp] = lax.dot_general(
        first_half, filtered, NT_DIMS, precision=exact, preferred_element_type=f32
    ) + lax.dot_general(
        1.0 - first_half, filtered * filtered, NT_DIMS, precision=exact, preferred_element_type=f32
    )

    def stat_copy(d):
        return pltpu.make_async_remote_copy(
            src_ref=stats.at[tp], dst_ref=stats.at[tp], send_sem=stat_s.at[d - 1], recv_sem=stat_r.at[d - 1],
            device_id={"tp": rem(tp + d, NX * NC)}, device_id_type=MESH,
        )

    def stat_arrival(d):
        slot = stats.at[rem(tp - d, NX * NC)]
        return pltpu.make_async_remote_copy(
            src_ref=slot, dst_ref=slot, send_sem=stat_s.at[d - 1], recv_sem=stat_r.at[d - 1],
            device_id={"tp": rem(tp + d, NX * NC)}, device_id_type=MESH,
        )

    for d in range(1, NX * NC):
        stat_copy(d).start()

    out_step(HALF + 3 - lag)
    for d in range(1, NX * NC):
        stat_arrival(d).wait_recv()
    totals = stats[0]
    for n in range(1, NX * NC):
        totals = totals + stats[n]
    scale = 1.0 / CONV_WIDTH
    row_id = lax.broadcasted_iota(jnp.int32, (8, cw), 0)
    mean = lax.dot_general(
        totals * scale, jnp.where(row_id == 0, 1.0, 0.0), TN_DIMS, precision=exact, preferred_element_type=f32
    )
    square = lax.dot_general(
        totals * scale, jnp.where(row_id == 4, 1.0, 0.0), TN_DIMS, precision=exact, preferred_element_type=f32
    )
    spread = jnp.maximum(square - mean * mean, 0.0)
    scaled = (filt[...] - mean) * lax.rsqrt(spread + 1e-05) * cgain[...]
    co[...] = (scaled * jax.nn.sigmoid(scaled)).astype(bf16)
    out_step(HALF + 4 - lag)
    block = 512

    def conv_part(j, carry):
        cols = pl.ds(pl.multiple_of(j * block, block), block)
        pc[:, cols] = lax.dot_general(co[...], oc[cols, :], NT_DIMS, preferred_element_type=f32)
        return carry

    lax.fori_loop(0, width // block, conv_part, 0)
    out_step(HALF + 5 - lag)
    for s in range(max(HALF + 6 - lag, 0), HALF + 3):
        out_step(s)
    for d in range(1, NZ):
        carry_copy(cz, rem(z - d, NZ), cz_s, cz_r, d, (z + d, y)).wait_recv()
    entering = jnp.zeros((1, half), f32)
    for n in range(NZ):
        entering = jnp.where(n < z, cz[n, :, :half] * entering + cz[n, :, half:], entering)
    entering = p_mine * entering + s_mine
    for g, (p_g, s_g) in enumerate(before):
        part = slice(g * seg, (g + 1) * seg)
        at_start = p_g * entering + s_g
        for n in range(n_tiles):
            used = min(tile, rw - n * tile)
            lanes = slice(n * tile, n * tile + used)
            state = ibuf[n, part, :used] + dbuf[n, part, :used] * at_start[:, lanes]
            ro[part, lanes] = (gbuf[part, lanes] * state).astype(bf16)

    def chip_rows(xx, cc):
        return pl.ds(pl.multiple_of((rem(xx, NX) * NC + rem(cc, NC)) * n_tok, n_tok), n_tok)

    def rec_part(j, carry):
        cols = pl.ds(pl.multiple_of(j * block, block), block)
        pc[:, cols] += lax.dot_general(ro[...], orr[cols, :rw], NT_DIMS, preferred_element_type=f32)
        for d in range(NX):
            ps[d, :, cols] = pc[chip_rows(x + d, c + 1), cols].astype(bf16)
        return carry

    quarter = width // 4

    def lanes_of(q):
        return slice(q * quarter, (q + 1) * quarter)

    def pair_copy(d, q):
        lanes = lanes_of(q)
        return pltpu.make_async_remote_copy(
            src_ref=ps.at[d, :, lanes], dst_ref=pr.at[d, :, lanes],
            send_sem=pr_s.at[4 * d + q], recv_sem=pr_r.at[4 * d + q],
            device_id={"tp": x * NC + rem(c + 1, NC)}, device_id_type=MESH,
        )

    def project(q):
        n_blocks = quarter // block
        lax.fori_loop(q * n_blocks, (q + 1) * n_blocks, rec_part, 0)
        for d in (2, 1, 3, 0):
            pair_copy(d, q).start()

    def x_copy(src, dst, index, q, xx):
        return pltpu.make_async_remote_copy(
            src_ref=src.at[:, lanes_of(q)], dst_ref=dst.at[:, lanes_of(q)],
            send_sem=x_s.at[index], recv_sem=x_r.at[index],
            device_id={"tp": rem(xx, NX) * NC + c}, device_id_type=MESH,
        )

    def chip_sum(d, q):
        pair_copy(d, q).wait_recv()
        return pc[chip_rows(x + d, c), lanes_of(q)] + pr[d, :, lanes_of(q)].astype(f32)

    far = [x_copy(s2, two, q, q, x + 1 if q < 2 else x - 1) for q in range(4)]
    up = [x_copy(sp_buf, from_m, 4 + q, q, x + 1) for q in range(4)]
    down = [x_copy(sm_buf, from_p, 8 + q, q, x - 1) for q in range(4)]

    def send_far(q):
        s2[:, lanes_of(q)] = chip_sum(2, q).astype(bf16)
        far[q].start()

    def send_near(d, q):
        buf, copies = (sp_buf, up) if d == 1 else (sm_buf, down)
        total = chip_sum(d, q)
        if (q < 2) == (d == 1):
            far[q].wait_recv()
            total = total + two[:, lanes_of(q)].astype(f32)
        buf[:, lanes_of(q)] = total.astype(bf16)
        copies[q].start()

    project(0)
    project(2)
    send_far(0)
    send_far(2)
    project(1)
    project(3)
    send_near(3, 0)
    send_near(1, 2)
    send_far(1)
    send_far(3)
    send_near(3, 1)
    send_near(1, 3)
    send_near(1, 0)
    send_near(3, 2)
    send_near(1, 1)
    send_near(3, 3)
    mine = chip_rows(x, c)
    for q in range(4):
        pc[mine, lanes_of(q)] = chip_sum(0, q)
    for q in (0, 2, 1, 3):
        at = lanes_of(q)
        up[q].wait_recv()
        down[q].wait_recv()
        out[:, at] = (pc[mine, at] + (from_m[:, at].astype(f32) + from_p[:, at].astype(f32))).astype(bf16)

    g_in.finish()
    g_out.finish()
    for args in t_sent:
        tok_copy(*args).wait_send()
    for e in edges:
        e.wait_send()
    for d in range(1, NX * NC):
        stat_copy(d).wait_send()
    for d in range(1, NY):
        carry_copy(cy, y, cy_s, cy_r, d, (z, y + d)).wait_send()
    for d in range(1, NZ):
        carry_copy(cz, z, cz_s, cz_r, d, (z + d, y)).wait_send()
    for q in range(4):
        for d in range(NX):
            pair_copy(d, q).wait_send()
    for n in far + up + down:
        n.wait_send()


def shards(
    tokens, norm_gain, conv_val_w, conv_gate_w, rec_gate_w, rec_in_w, conv_taps, conv_bias, conv_gain,
    short_taps, decay_map, input_map, decay_base, decay_jump, out_conv_w, out_rec_w,
):
    cw, rw = conv_val_w.shape[1], rec_in_w.shape[1]
    n_tok, width = tokens.shape
    length = n_tok * NX * NC
    wide = rw + -rw % 128
    f32, bf16 = jnp.float32, jnp.bfloat16
    vmem = pl.BlockSpec(memory_space=pltpu.VMEM)
    V, S = pltpu.VMEM, pltpu.SemaphoreType.DMA
    return pl.pallas_call(
        whole_kernel,
        out_shape=jax.ShapeDtypeStruct((n_tok, width), bf16),
        in_specs=[vmem] * 16,
        out_specs=vmem,
        scratch_shapes=[
            V((length, width), bf16),
            V((width, 2 * cw), bf16),
            V((width, 2 * rw), bf16),
            V((length, 2 * cw), f32),
            V((length, 2 * rw), f32),
            V((width, cw), bf16),
            V((width * 3 // 2, 128), bf16),
            V((width, wide), bf16),
            V((length + 32, cw), f32),
            V((length + 8, rw), f32),
            V((length, cw), f32),
            V((rw, rw), bf16),
            V((rw, rw), bf16),
            V((NX * NC, 8, length), f32),
            V((wide // 128, length, 128), f32),
            V((wide // 128, length, 128), f32),
            V((length, rw), f32),
            V((length, cw), bf16),
            V((length, rw), bf16),
            V((length, rw), f32),
            V((NY, 1, 2 * wide), f32),
            V((NZ, 1, 2 * wide), f32),
            V((length, width), f32),
            V((NX, n_tok, width), bf16),
            V((NX, n_tok, width), bf16),
            V((n_tok, width), bf16),
            V((n_tok, width), bf16),
            V((n_tok, width), bf16),
            V((n_tok, width), bf16),
            V((n_tok, width), bf16),
            V((n_tok, width), bf16),
            *Gather.semaphores(),
            *Gather.semaphores(),
            S((9,)), S((9,)), S((2,)), S((2,)), S((7,)), S((7,)), S((3,)), S((3,)),
            S((NZ - 1,)), S((NZ - 1,)), S((4 * NX,)), S((4 * NX,)), S((12,)), S((12,)),
        ],
        compiler_params=pltpu.CompilerParams(
            collective_id=0, has_side_effects=True, vmem_limit_bytes=60 * 1024 * 1024
        ),
    )(
        tokens,
        norm_gain[None, :],
        conv_val_w,
        conv_gate_w,
        rec_in_w,
        rec_gate_w,
        out_conv_w.T,
        out_rec_w.T,
        conv_taps,
        conv_bias[None, :],
        conv_gain[None, :],
        short_taps,
        decay_map,
        input_map,
        decay_base[None, :],
        decay_jump.T,
    )


def solution(mesh):
    in_specs = (
        P(("sp", "tp"), None), P(), P("sp", "tp"), P("sp", "tp"), P("sp", "tp"), P("sp", "tp"),
        P(None, "tp"), P("tp"), P("tp"), P(None, "tp"), P("tp", None, None), P("tp", None, None),
        P("tp"), P("sp", "tp"), P("tp", "sp"), P("tp", "sp"),
    )
    return jax.shard_map(
        shards, mesh=mesh, in_specs=in_specs, out_specs=P(("sp", "tp"), None), check_vma=False
    )
```

```python
import jax
import jax.numpy as jnp
from jax import lax
from jax.experimental import pallas as pl
from jax.experimental.pallas import tpu as pltpu
from jax.sharding import PartitionSpec as P

MESH = pl.DeviceIdType.MESH
CONV_WIDTH = 1024
RATE_SCALE = 8.0
NZ, NY, NX, NC = 16, 4, 4, 2
HALF = NZ // 2


def rem(a, n):
    return lax.rem(a + 4 * n, n)


class Gather:
    def __init__(self, a, b, rows, sems, pos):
        self.a, self.b = a, b
        self.rows = {id(a): rows[0], id(b): rows[1]}
        self.s, self.r = {id(a): sems[0], id(b): sems[1]}, sems[2:]
        self.z, self.y = pos
        self.sent = {id(a): 0, id(b): 0}

    def at(self, ref, z, y):
        rows = self.rows[id(ref)]
        return ref.at[pl.ds(pl.multiple_of((rem(z, NZ) * NY + rem(y, NY)) * rows, rows), rows)]

    def copy(self, ref, chunk, kind, index, to):
        block = self.at(ref, *chunk)
        return pltpu.make_async_remote_copy(
            src_ref=block,
            dst_ref=block,
            send_sem=self.s[id(ref)].at[0],
            recv_sem=self.r[kind].at[index],
            device_id={"sp": rem(to[0], NZ) * NY + rem(to[1], NY)},
            device_id_type=MESH,
        )

    def send(self, *args):
        self.copy(*args).start()
        self.sent[id(args[0])] += 1

    def arrived(self, ref, chunk, kind, index):
        self.copy(ref, chunk, kind, index, (self.z + 1, self.y)).wait_recv()

    def start_y(self):
        z, y, a = self.z, self.y, self.a
        for d in (1, 3, 2):
            self.send(a, (z, y), 0, d - 1, (z, y + d))

    def start_z(self):
        z, y = self.z, self.y
        for ref, up in ((self.b, 3), (self.a, 1)):
            self.send(ref, (z, y), up, 0, (z + 1, y))
            self.send(ref, (z, y), up + 1, 0, (z - 1, y))

    def from_y(self):
        z, y, a = self.z, self.y, self.a
        for d in (1, 3, 2):
            self.arrived(a, (z, y - d), 0, d - 1)
            self.send(a, (z, y - d), 1, d, (z + 1, y))
            self.send(a, (z, y - d), 2, d, (z - 1, y))

    def spread(self, k):
        z, y = self.z, self.y
        self.send(self.b, (z - k, y), 5, 3 * k, (z, y + 1))
        self.send(self.b, (z - k, y), 5, 3 * k + 1, (z, y - 1))
        if k == HALF:
            self.send(self.b, (z - k, y), 5, 3 * k + 2, (z, y + 2))

    def along_z(self, s, between=lambda: None):
        z, y, a, b = self.z, self.y, self.a, self.b
        last = s == HALF
        self.arrived(b, (z - s, y), 3, s - 1)
        if not last:
            self.send(b, (z - s, y), 3, s, (z + 1, y))
        if not last:
            self.arrived(b, (z + s, y), 4, s - 1)
            if s + 1 < HALF:
                self.send(b, (z + s, y), 4, s, (z - 1, y))
        self.spread(s)
        if not last:
            self.spread(NZ - s)
        for d in (0, 1, 3, 2):
            if not last or d == 0:
                self.arrived(a, (z - s, y - d), 1, 4 * (s - 1) + d)
                if s + 1 < HALF or s + 1 == HALF and d == 0:
                    self.send(a, (z - s, y - d), 1, 4 * s + d, (z + 1, y))
            if not last or d > 0:
                self.arrived(a, (z + s, y - d), 2, 4 * (s - 1) + d)
                if s + 1 < HALF or s + 1 == HALF and d > 0:
                    self.send(a, (z + s, y - d), 2, 4 * s + d, (z - 1, y))
            between()

    def along_y(self, k):
        z, y = self.z, self.y
        turn = 1 - 2 * (k % 2)
        self.arrived(self.b, (z - k, y - 1), 5, 3 * k)
        self.arrived(self.b, (z - k, y + 1), 5, 3 * k + 1)
        if k != HALF:
            self.send(self.b, (z - k, y - turn), 5, 3 * k + 2, (z, y + turn))

    def along_y_last(self, k):
        self.arrived(self.b, (self.z - k, self.y + 2), 5, 3 * k + 2)

    def finish(self):
        for ref in (self.a, self.b):
            everything = ref.at[pl.ds(0, self.sent[id(ref)] * self.rows[id(ref)])]
            pltpu.make_async_remote_copy(
                src_ref=everything, dst_ref=everything, send_sem=self.s[id(ref)].at[0], recv_sem=self.r[0].at[0],
                device_id={"sp": rem(self.z + 1, NZ) * NY + self.y}, device_id_type=MESH,
            ).wait_send()

    @staticmethod
    def semaphores():
        counts = [1, 1, 3, 4 * HALF, 4 * HALF, HALF, HALF, 3 * NZ]
        return [pltpu.SemaphoreType.DMA((n,)) for n in counts]


N_SEMS = 8


def groups_of(step):
    if step == 0:
        return [0]
    if step < HALF:
        return [step, NZ - step]
    return [step] if step == HALF else []


def expm1_negated(v):
    series = jnp.ones_like(v)
    for n in range(9, 1, -1):
        series = 1.0 + series * v * (1.0 / n)
    return jnp.where(v > -0.5, -v * series, 1.0 - jnp.exp(v))


def softplus_negated(b):
    e = jnp.exp(-jnp.abs(b))
    w = e / (2.0 + e)
    q = w * w
    series = jnp.full_like(w, 1.0 / 15.0)
    for n in (13, 11, 9, 7, 5, 3, 1):
        series = 1.0 / n + series * q
    return jnp.maximum(-b, 0.0) + 2.0 * w * series


NT_DIMS = (((1,), (1,)), ((), ()))
TN_DIMS = (((0,), (0,)), ((), ()))
SEGS = 8


def whole_kernel(
    tokens, gain, wv_own, wg_own, ri_own, rg_own, oc_own, or_own, taps, bias, cgain, staps, dmap, imap, base, jump_t, out, *scratch
):
    (nt, wa, wb, acc_a, acc_b, oc, packed, orr, ext_c, ext_r, filt, md, mi, stats, dbuf, ibuf, gbuf, co, ro,
     jump, cy, cz, pc, ps, pr, s2, sp_buf, sm_buf, two, from_m, from_p) = scratch[:31]
    scratch = scratch[31:]
    sems_in, sems_out = scratch[:N_SEMS], scratch[N_SEMS : 2 * N_SEMS]
    (tok_s, tok_r, edge_s, edge_r, stat_s, stat_r, cy_s, cy_r, cz_s, cz_r, pr_s, pr_r, x_s, x_r) = scratch[2 * N_SEMS :]
    sp, tp = lax.axis_index("sp"), lax.axis_index("tp")
    z, y, x, c = sp // NY, sp % NY, tp // NC, tp % NC
    rows = wv_own.shape[0]
    n_tok, width = tokens.shape
    length = acc_a.shape[0]
    cw, rw = wv_own.shape[1], ri_own.shape[1]
    f32, bf16 = jnp.float32, jnp.bfloat16

    barrier = pltpu.get_barrier_semaphore()
    for dz, dy in ((1, 0), (-1, 0), (0, 1), (0, 2), (0, 3)):
        pl.semaphore_signal(
            barrier, inc=1, device_id={"sp": rem(z + dz, NZ) * NY + rem(y + dy, NY)}, device_id_type=MESH
        )
    for d in (1, -1):
        pl.semaphore_signal(barrier, inc=1, device_id={"sp": rem(sp + d, NZ * NY)}, device_id_type=MESH)
    for d in range(1, NX * NC):
        pl.semaphore_signal(barrier, inc=1, device_id={"tp": rem(tp + d, NX * NC)}, device_id_type=MESH)

    own = pl.ds(pl.multiple_of(sp * rows, rows), rows)
    extra = wa.shape[1] - rw
    wa[own, :] = jnp.concatenate([ri_own[...], rg_own[:, :extra]], axis=1)
    wb[own, :cw] = wv_own[...]
    wb[own, cw : 2 * cw] = wg_own[...]
    wb[own, 2 * cw :] = rg_own[:, extra:]
    oc[own] = oc_own[...]
    p_rows, h_rows = rows + rows // 2, rows // 2
    p_at = pl.multiple_of(sp * p_rows, h_rows)
    packed[pl.ds(p_at, rows)] = or_own[:, :128]
    packed[pl.ds(p_at + rows, h_rows)] = jnp.concatenate([or_own[:h_rows, 128:], or_own[h_rows:, 128:]], axis=1)

    def unpack(k):
        for n in range(NY):
            chunk = rem(z - k, NZ) * NY + n
            src = pl.multiple_of(chunk * p_rows, h_rows)
            dst = pl.multiple_of(chunk * rows, rows)
            orr[pl.ds(dst, rows), :128] = packed[pl.ds(src, rows)]
            pair = packed[pl.ds(src + rows, h_rows)]
            orr[pl.ds(dst, h_rows), 128:rw] = pair[:, : rw - 128]
            orr[pl.ds(dst + h_rows, h_rows), 128:rw] = pair[:, rw - 128 :]

    pl.semaphore_wait(barrier, 7 + NX * NC - 1)

    g_in = Gather(wa, wb, (rows, rows), sems_in, (z, y))
    g_out = Gather(oc, packed, (rows, rows + rows // 2), sems_out, (z, y))
    g_in.start_z()
    g_in.start_y()
    g_in.spread(0)
    g_out.start_z()

    def tok_rows(xx, cc):
        return pl.ds(pl.multiple_of((rem(xx, NX) * NC + rem(cc, NC)) * n_tok, 16), n_tok)

    def tok_at(xx, cc, lanes=None):
        r = tok_rows(xx, cc)
        return nt.at[r] if lanes is None else nt.at[r, lanes]

    def tok_copy(block, index, xx, cc):
        return pltpu.make_async_remote_copy(
            src_ref=block, dst_ref=block, send_sem=tok_s.at[0], recv_sem=tok_r.at[index],
            device_id={"tp": rem(xx, NX) * NC + rem(cc, NC)}, device_id_type=MESH,
        )

    def tok_send(*args):
        tok_copy(*args).start()

    lo, hi = pl.ds(0, width // 2), pl.ds(width // 2, width // 2)

    widened = tokens[...].astype(f32)
    inverse = lax.rsqrt(jnp.mean(widened * widened, axis=-1, keepdims=True) + 1e-06)
    tok_at(x, c)[...] = (widened * inverse * gain[...]).astype(bf16)
    tok_send(tok_at(x, c), 0, x + 1, c)
    tok_send(tok_at(x, c), 1, x - 1, c)
    tok_send(tok_at(x, c), 4, x, c + 1)
    g_in.from_y()
    g_out.start_y()
    acc_a[...] = jnp.zeros_like(acc_a)
    acc_b[...] = jnp.zeros_like(acc_b)
    cy[...] = jnp.zeros_like(cy)
    cz[...] = jnp.zeros_like(cz)
    head = dmap.shape[1]
    for m, given in ((md, dmap), (mi, imap)):
        m[...] = jnp.zeros_like(m)
        for h in range(dmap.shape[0]):
            m[h * head : (h + 1) * head, h * head : (h + 1) * head] = given[h]
    jump[...] = jnp.transpose(jump_t[...])

    def tokens_forward():
        tok_copy(tok_at(x - 1, c), 0, x + 1, c).wait_recv()
        tok_send(tok_at(x - 1, c, lo), 2, x + 1, c)
        tok_send(tok_at(x - 1, c), 5, x, c + 1)
        tok_copy(tok_at(x + 1, c), 1, x + 1, c).wait_recv()
        tok_send(tok_at(x + 1, c, hi), 3, x - 1, c)
        tok_send(tok_at(x + 1, c), 6, x, c + 1)

    def tokens_relay():
        tok_copy(tok_at(x + 2, c, lo), 2, x + 1, c).wait_recv()
        tok_send(tok_at(x + 2, c, lo), 7, x, c + 1)
        tok_copy(tok_at(x + 2, c, hi), 3, x + 1, c).wait_recv()
        tok_send(tok_at(x + 2, c, hi), 8, x, c + 1)

    def tokens_last():
        tok_copy(tok_at(x, c + 1), 4, x + 1, c).wait_recv()
        tok_copy(tok_at(x - 1, c + 1), 5, x + 1, c).wait_recv()
        tok_copy(tok_at(x + 1, c + 1), 6, x + 1, c).wait_recv()
        tok_copy(tok_at(x + 2, c + 1, lo), 7, x + 1, c).wait_recv()
        tok_copy(tok_at(x + 2, c + 1, hi), 8, x + 1, c).wait_recv()

    def multiply(acc, w, first, last):
        def body(j, carry):
            s = (j + 1) // 2
            zz = rem(z + jnp.where(j % 2 == 1, -s, s), NZ)
            cols = pl.ds(pl.multiple_of(zz * (NY * rows), NY * rows), NY * rows)
            acc[...] += jnp.dot(nt[:, cols], w[cols, :], preferred_element_type=f32)
            return carry

        lax.fori_loop(first, last, body, 0)

    a_part = lambda first, last: (lambda: multiply(acc_a, wa, first, last))
    b_part = lambda first, last: (lambda: multiply(acc_b, wb, first, last))
    work = {
        6: [a_part(0, 2), a_part(2, 4), a_part(4, 6), a_part(6, 8)],
        7: [a_part(8, 10), a_part(10, 12), b_part(0, 2), b_part(2, 4)],
        8: [b_part(4, 6), b_part(6, 8), b_part(8, 10), a_part(12, 15)],
    }

    def out_step(s):
        if s == 0:
            g_out.spread(0)
            g_out.from_y()
        elif s <= HALF:
            g_out.along_z(s)
        if s >= 1:
            for k in groups_of(s - 1):
                g_out.along_y(k)
        if s >= 2:
            for k in groups_of(s - 2):
                g_out.along_y_last(k)
                unpack(k)

    lag = 3

    def at_step(step):
        todo = list(work.get(step, []))
        g_in.along_z(step, lambda: todo and todo.pop(0)())
        if step == HALF:
            a_part(NZ - 1, NZ)()
            start_recurrence()
        for k in groups_of(step - 1):
            g_in.along_y(k)
        if step >= lag:
            out_step(step - lag)
        if step >= 2:
            for k in groups_of(step - 2):
                g_in.along_y_last(k)
        if step == 2:
            tokens_forward()
        if step == 4:
            tokens_relay()
        if step == 5:
            tokens_last()

    c_pad, r_pad = ext_c.shape[0] - length, ext_r.shape[0] - length

    def edge_copy(ref, pad, index):
        return pltpu.make_async_remote_copy(
            src_ref=ref.at[pl.ds(length, pad)], dst_ref=ref.at[pl.ds(0, pad)],
            send_sem=edge_s.at[index], recv_sem=edge_r.at[index],
            device_id={"sp": rem(sp + 1, NZ * NY)}, device_id_type=MESH,
        )

    edges = [edge_copy(ext_r, r_pad, 0), edge_copy(ext_c, c_pad, 1)]

    def take_edge(index, ref, pad):
        edges[index].wait_recv()
        ref[:pad, :] = jnp.where(sp > 0, ref[:pad, :], 0.0)

    def start_recurrence():
        ext_r[r_pad:, :] = acc_a[:, :rw].astype(bf16).astype(f32)
        edges[0].start()

    for step in range(1, HALF + 1):
        at_step(step)

    n_short = staps.shape[0]
    short = staps[...].astype(f32)
    rate = -RATE_SCALE * softplus_negated(base[...])
    tile = 128
    n_tiles = dbuf.shape[0]

    def gates(first, count):
        smoothed = jnp.zeros((count, rw), f32)
        for k in range(n_short):
            at = r_pad - (n_short - 1) + k + first
            smoothed = smoothed + short[k : k + 1, :] * ext_r[at : at + count, :]
        rounded = smoothed.astype(bf16)
        retain = jax.nn.sigmoid(jnp.dot(rounded, md[...], preferred_element_type=f32))
        admit = jax.nn.sigmoid(jnp.dot(rounded, mi[...], preferred_element_type=f32))
        log_decay = rate * retain + jump[first : first + count, :]
        decay = jnp.exp(log_decay)
        inflow = jnp.sqrt(expm1_negated(2.0 * log_decay)) * admit * rounded.astype(f32)
        for n in range(n_tiles):
            used = min(tile, rw - n * tile)
            dbuf[n, first : first + count, :used] = decay[:, n * tile : n * tile + used]
            ibuf[n, first : first + count, :used] = inflow[:, n * tile : n * tile + used]

    early = 16
    gates(early, length - early)
    b_part(10, 13)()
    take_edge(0, ext_r, r_pad)
    gates(0, early)
    seg = length // SEGS

    def scan_step(j, carry):
        new = []
        for n, (p, s) in enumerate(carry):
            at = (n, pl.ds(j, SEGS, stride=seg), slice(None))
            d, i = dbuf[at], ibuf[at]
            p, s = d * p, d * s + i
            dbuf[at] = p
            ibuf[at] = s
            new.append((p, s))
        return tuple(new)

    start = tuple((jnp.ones((SEGS, tile), f32), jnp.zeros((SEGS, tile), f32)) for _ in range(n_tiles))
    ends = lax.fori_loop(0, seg, scan_step, start)
    p_all = jnp.concatenate([e[0] for e in ends], axis=1)
    s_all = jnp.concatenate([e[1] for e in ends], axis=1)
    half = cy.shape[2] // 2
    p_run, s_run = jnp.ones((1, half), f32), jnp.zeros((1, half), f32)
    before = []
    for g in range(SEGS):
        before.append((p_run, s_run))
        p_g, s_g = p_all[g : g + 1, :], s_all[g : g + 1, :]
        p_run, s_run = p_run * p_g, p_g * s_run + s_g

    def carry_copy(buf, slot, send, recv, to):
        return pltpu.make_async_remote_copy(
            src_ref=buf.at[slot], dst_ref=buf.at[slot], send_sem=send.at[0], recv_sem=recv.at[0],
            device_id={"sp": rem(to[0], NZ) * NY + rem(to[1], NY)}, device_id_type=MESH,
        )

    cy[y, :, :half] = p_run
    cy[y, :, half:] = s_run
    for d in range(1, NY):
        carry_copy(cy, pl.ds(y, 1), cy_s, cy_r, (z, y + d)).start()
    out_step(HALF + 1 - lag)
    for k in groups_of(HALF):
        g_in.along_y(k)
    for k in groups_of(HALF - 1) + groups_of(HALF):
        g_in.along_y_last(k)
    b_part(13, NZ)()
    conv_val = acc_b[:, :cw].astype(bf16).astype(f32)
    conv_gate = acc_b[:, cw : 2 * cw].astype(bf16).astype(f32)
    ext_c[c_pad:, :] = (conv_val * jax.nn.sigmoid(conv_gate)).astype(bf16).astype(f32)
    edges[1].start()
    gate = jnp.concatenate([acc_a[:, rw:], acc_b[:, 2 * cw :]], axis=1).astype(bf16).astype(f32)
    gbuf[...] = 0.5 * gate * (1.0 + jnp.tanh(0.7978845608028654 * (gate + 0.044715 * gate * gate * gate)))
    carry_copy(cy, pl.ds(0, NY - 1), cy_s, cy_r, (z, y + 1)).wait_recv()
    p_run, s_run = jnp.ones((1, half), f32), jnp.zeros((1, half), f32)
    p_mine, s_mine = p_run, s_run
    for n in range(NY):
        p_mine = jnp.where(y == n, p_run, p_mine)
        s_mine = jnp.where(y == n, s_run, s_mine)
        p_n, s_n = cy[n, :, :half], cy[n, :, half:]
        p_run, s_run = p_run * p_n, p_n * s_run + s_n
    cz[z, :, :half] = p_run
    cz[z, :, half:] = s_run
    for d in range(1, NZ):
        carry_copy(cz, pl.ds(z, 1), cz_s, cz_r, (z + d, y)).start()
    out_step(HALF + 2 - lag)
    n_taps = taps.shape[0]
    wide = taps[...].astype(f32)
    tap_rows = 32

    def filter_rows(first):
        total = jnp.broadcast_to(bias[...], (tap_rows, cw))
        for k in range(n_taps):
            at = first + c_pad - (n_taps - 1) + k
            total = total + wide[k : k + 1, :] * ext_c[at : at + tap_rows, :]
        filt[first : first + tap_rows, :] = total

    for i in range(1, length // tap_rows):
        filter_rows(i * tap_rows)
    take_edge(1, ext_c, c_pad)
    filter_rows(0)
    filtered = filt[...]
    row_id = lax.broadcasted_iota(jnp.int32, (8, cw), 0)
    first_half = jnp.where(row_id < 4, 1.0, 0.0)
    exact = lax.Precision.HIGHEST
    stats[tp] = lax.dot_general(
        first_half, filtered, NT_DIMS, precision=exact, preferred_element_type=f32
    ) + lax.dot_general(
        1.0 - first_half, filtered * filtered, NT_DIMS, precision=exact, preferred_element_type=f32
    )

    def stat_copy(d):
        return pltpu.make_async_remote_copy(
            src_ref=stats.at[tp], dst_ref=stats.at[tp], send_sem=stat_s.at[0], recv_sem=stat_r.at[0],
            device_id={"tp": rem(tp + d, NX * NC)}, device_id_type=MESH,
        )

    stats_of_others = pltpu.make_async_remote_copy(
        src_ref=stats.at[pl.ds(0, NX * NC - 1)], dst_ref=stats.at[pl.ds(0, NX * NC - 1)],
        send_sem=stat_s.at[0], recv_sem=stat_r.at[0],
        device_id={"tp": rem(tp + 1, NX * NC)}, device_id_type=MESH,
    )

    for d in range(1, NX * NC):
        stat_copy(d).start()

    out_step(HALF + 3 - lag)
    stats_of_others.wait_recv()
    totals = stats[0]
    for n in range(1, NX * NC):
        totals = totals + stats[n]
    scale = 1.0 / CONV_WIDTH
    row_id = lax.broadcasted_iota(jnp.int32, (8, cw), 0)
    mean = lax.dot_general(
        totals * scale, jnp.where(row_id == 0, 1.0, 0.0), TN_DIMS, precision=exact, preferred_element_type=f32
    )
    square = lax.dot_general(
        totals * scale, jnp.where(row_id == 4, 1.0, 0.0), TN_DIMS, precision=exact, preferred_element_type=f32
    )
    spread = jnp.maximum(square - mean * mean, 0.0)
    scaled = (filt[...] - mean) * lax.rsqrt(spread + 1e-05) * cgain[...]
    co[...] = (scaled * jax.nn.sigmoid(scaled)).astype(bf16)
    out_step(HALF + 4 - lag)
    out_step(HALF + 5 - lag)
    for s in range(max(HALF + 6 - lag, 0), HALF + 3):
        out_step(s)
    carry_copy(cz, pl.ds(0, NZ - 1), cz_s, cz_r, (z + 1, y)).wait_recv()
    entering = jnp.zeros((1, half), f32)
    for n in range(NZ):
        entering = jnp.where(n < z, cz[n, :, :half] * entering + cz[n, :, half:], entering)
    entering = p_mine * entering + s_mine
    for g, (p_g, s_g) in enumerate(before):
        part = slice(g * seg, (g + 1) * seg)
        at_start = p_g * entering + s_g
        for n in range(n_tiles):
            used = min(tile, rw - n * tile)
            lanes = slice(n * tile, n * tile + used)
            state = ibuf[n, part, :used] + dbuf[n, part, :used] * at_start[:, lanes]
            ro[part, lanes] = (gbuf[part, lanes] * state).astype(bf16)

    def chip_rows(xx, cc):
        return pl.ds(pl.multiple_of((rem(xx, NX) * NC + rem(cc, NC)) * n_tok, n_tok), n_tok)

    block = 512

    def out_part(j, carry):
        cols = pl.ds(pl.multiple_of(j * block, block), block)
        pc[:, cols] = lax.dot_general(
            co[...], oc[cols, :], NT_DIMS, preferred_element_type=f32
        ) + lax.dot_general(ro[...], orr[cols, :rw], NT_DIMS, preferred_element_type=f32)
        for d in range(NX):
            ps[d, :, cols] = pc[chip_rows(x + d, c + 1), cols].astype(bf16)
        return carry

    quarter = width // 4

    def lanes_of(q):
        return slice(q * quarter, (q + 1) * quarter)

    def pair_copy(d, q):
        lanes = lanes_of(q)
        return pltpu.make_async_remote_copy(
            src_ref=ps.at[d, :, lanes], dst_ref=pr.at[d, :, lanes],
            send_sem=pr_s.at[0], recv_sem=pr_r.at[4 * d + q],
            device_id={"tp": x * NC + rem(c + 1, NC)}, device_id_type=MESH,
        )

    def project(q):
        n_blocks = quarter // block
        lax.fori_loop(q * n_blocks, (q + 1) * n_blocks, out_part, 0)
        for d in (2, 1, 3, 0):
            pair_copy(d, q).start()

    def x_copy(src, dst, index, q, xx):
        return pltpu.make_async_remote_copy(
            src_ref=src.at[:, lanes_of(q)], dst_ref=dst.at[:, lanes_of(q)],
            send_sem=x_s.at[index // 4], recv_sem=x_r.at[index],
            device_id={"tp": rem(xx, NX) * NC + c}, device_id_type=MESH,
        )

    def chip_sum(d, q):
        pair_copy(d, q).wait_recv()
        return pc[chip_rows(x + d, c), lanes_of(q)] + pr[d, :, lanes_of(q)].astype(f32)

    far = [x_copy(s2, two, q, q, x + 1 if q < 2 else x - 1) for q in range(4)]
    up = [x_copy(sp_buf, from_m, 4 + q, q, x + 1) for q in range(4)]
    down = [x_copy(sm_buf, from_p, 8 + q, q, x - 1) for q in range(4)]

    def send_far(q):
        s2[:, lanes_of(q)] = chip_sum(2, q).astype(bf16)
        far[q].start()

    def send_near(d, q):
        buf, copies = (sp_buf, up) if d == 1 else (sm_buf, down)
        total = chip_sum(d, q)
        if (q < 2) == (d == 1):
            far[q].wait_recv()
            total = total + two[:, lanes_of(q)].astype(f32)
        buf[:, lanes_of(q)] = total.astype(bf16)
        copies[q].start()

    project(0)
    project(2)
    send_far(0)
    send_far(2)
    project(1)
    project(3)
    send_near(3, 0)
    send_near(1, 2)
    send_far(1)
    send_far(3)
    send_near(3, 1)
    send_near(1, 3)
    send_near(1, 0)
    send_near(3, 2)
    send_near(1, 1)
    send_near(3, 3)
    mine = chip_rows(x, c)
    for q in range(4):
        pc[mine, lanes_of(q)] = chip_sum(0, q)
    for q in (0, 2, 1, 3):
        at = lanes_of(q)
        up[q].wait_recv()
        down[q].wait_recv()
        out[:, at] = (pc[mine, at] + (from_m[:, at].astype(f32) + from_p[:, at].astype(f32))).astype(bf16)

    g_in.finish()
    g_out.finish()
    tok_copy(nt.at[pl.ds(0, 7 * n_tok)], 0, x + 1, c).wait_send()
    for e in edges:
        e.wait_send()
    stats_of_others.wait_send()
    carry_copy(cy, pl.ds(0, NY - 1), cy_s, cy_r, (z, y + 1)).wait_send()
    carry_copy(cz, pl.ds(0, NZ - 1), cz_s, cz_r, (z + 1, y)).wait_send()
    pltpu.make_async_remote_copy(
        src_ref=ps, dst_ref=pr, send_sem=pr_s.at[0], recv_sem=pr_r.at[0],
        device_id={"tp": x * NC + rem(c + 1, NC)}, device_id_type=MESH,
    ).wait_send()
    for n, buf in enumerate((s2, sp_buf, sm_buf)):
        pltpu.make_async_remote_copy(
            src_ref=buf, dst_ref=two, send_sem=x_s.at[n], recv_sem=x_r.at[0],
            device_id={"tp": rem(x + 1, NX) * NC + c}, device_id_type=MESH,
        ).wait_send()


def shards(
    tokens, norm_gain, conv_val_w, conv_gate_w, rec_gate_w, rec_in_w, conv_taps, conv_bias, conv_gain,
    short_taps, decay_map, input_map, decay_base, decay_jump, out_conv_w, out_rec_w,
):
    cw, rw = conv_val_w.shape[1], rec_in_w.shape[1]
    n_tok, width = tokens.shape
    length = n_tok * NX * NC
    wide = rw + -rw % 128
    f32, bf16 = jnp.float32, jnp.bfloat16
    vmem = pl.BlockSpec(memory_space=pltpu.VMEM)
    V, S = pltpu.VMEM, pltpu.SemaphoreType.DMA
    return pl.pallas_call(
        whole_kernel,
        out_shape=jax.ShapeDtypeStruct((n_tok, width), bf16),
        in_specs=[vmem] * 16,
        out_specs=vmem,
        scratch_shapes=[
            V((length, width), bf16),
            V((width, 2 * cw), bf16),
            V((width, 2 * rw), bf16),
            V((length, 2 * cw), f32),
            V((length, 2 * rw), f32),
            V((width, cw), bf16),
            V((width * 3 // 2, 128), bf16),
            V((width, wide), bf16),
            V((length + 32, cw), f32),
            V((length + 8, rw), f32),
            V((length, cw), f32),
            V((rw, rw), bf16),
            V((rw, rw), bf16),
            V((NX * NC, 8, length), f32),
            V((wide // 128, length, 128), f32),
            V((wide // 128, length, 128), f32),
            V((length, rw), f32),
            V((length, cw), bf16),
            V((length, rw), bf16),
            V((length, rw), f32),
            V((NY, 1, 2 * wide), f32),
            V((NZ, 1, 2 * wide), f32),
            V((length, width), f32),
            V((NX, n_tok, width), bf16),
            V((NX, n_tok, width), bf16),
            V((n_tok, width), bf16),
            V((n_tok, width), bf16),
            V((n_tok, width), bf16),
            V((n_tok, width), bf16),
            V((n_tok, width), bf16),
            V((n_tok, width), bf16),
            *Gather.semaphores(),
            *Gather.semaphores(),
            S((1,)), S((9,)), S((2,)), S((2,)), S((1,)), S((1,)), S((1,)), S((1,)),
            S((1,)), S((1,)), S((1,)), S((4 * NX,)), S((3,)), S((12,)),
        ],
        compiler_params=pltpu.CompilerParams(
            collective_id=0, has_side_effects=True, vmem_limit_bytes=60 * 1024 * 1024
        ),
    )(
        tokens,
        norm_gain[None, :],
        conv_val_w,
        conv_gate_w,
        rec_in_w,
        rec_gate_w,
        out_conv_w.T,
        out_rec_w.T,
        conv_taps,
        conv_bias[None, :],
        conv_gain[None, :],
        short_taps,
        decay_map,
        input_map,
        decay_base[None, :],
        decay_jump.T,
    )


def solution(mesh):
    in_specs = (
        P(("sp", "tp"), None), P(), P("sp", "tp"), P("sp", "tp"), P("sp", "tp"), P("sp", "tp"),
        P(None, "tp"), P("tp"), P("tp"), P(None, "tp"), P("tp", None, None), P("tp", None, None),
        P("tp"), P("sp", "tp"), P("tp", "sp"), P("tp", "sp"),
    )
    return jax.shard_map(
        shards, mesh=mesh, in_specs=in_specs, out_specs=P(("sp", "tp"), None), check_vma=False
    )
```

```python
import jax
import jax.numpy as jnp
from jax import lax
from jax.experimental import pallas as pl
from jax.experimental.pallas import tpu as pltpu
from jax.sharding import PartitionSpec as P

MESH = pl.DeviceIdType.MESH
CONV_WIDTH = 1024
RATE_SCALE = 8.0
NZ, NY, NX, NC = 16, 4, 4, 2
HALF = NZ // 2


def rem(a, n):
    return lax.rem(a + 4 * n, n)


class Gather:
    def __init__(self, a, b, rows, sems, pos):
        self.a, self.b = a, b
        self.rows = {id(a): rows[0], id(b): rows[1]}
        self.s, self.r = {id(a): sems[0], id(b): sems[1]}, sems[2:]
        self.z, self.y = pos
        self.sent = {id(a): 0, id(b): 0}

    def at(self, ref, z, y):
        rows = self.rows[id(ref)]
        return ref.at[pl.ds(pl.multiple_of((rem(z, NZ) * NY + rem(y, NY)) * rows, rows), rows)]

    def copy(self, ref, chunk, kind, index, to):
        block = self.at(ref, *chunk)
        return pltpu.make_async_remote_copy(
            src_ref=block,
            dst_ref=block,
            send_sem=self.s[id(ref)].at[0],
            recv_sem=self.r[kind].at[index],
            device_id={"sp": rem(to[0], NZ) * NY + rem(to[1], NY)},
            device_id_type=MESH,
        )

    def send(self, *args):
        self.copy(*args).start()
        self.sent[id(args[0])] += 1

    def arrived(self, ref, chunk, kind, index):
        self.copy(ref, chunk, kind, index, (self.z + 1, self.y)).wait_recv()

    def start_y(self):
        z, y, a = self.z, self.y, self.a
        for d in (1, 3, 2):
            self.send(a, (z, y), 0, d - 1, (z, y + d))

    def start_z(self):
        z, y = self.z, self.y
        for ref, up in ((self.b, 3), (self.a, 1)):
            self.send(ref, (z, y), up, 0, (z + 1, y))
            self.send(ref, (z, y), up + 1, 0, (z - 1, y))

    def from_y(self):
        z, y, a = self.z, self.y, self.a
        for d in (1, 3, 2):
            self.arrived(a, (z, y - d), 0, d - 1)
            self.send(a, (z, y - d), 1, d, (z + 1, y))
            self.send(a, (z, y - d), 2, d, (z - 1, y))

    def spread(self, k):
        z, y = self.z, self.y
        self.send(self.b, (z - k, y), 5, 2 * k, (z, y + 1))
        self.send(self.b, (z - k, y), 5, 2 * k, (z, y - 1))
        if k == HALF:
            self.send(self.b, (z - k, y), 5, 2 * k + 1, (z, y + 2))

    def along_z(self, s, between=lambda: None):
        z, y, a, b = self.z, self.y, self.a, self.b
        last = s == HALF
        self.arrived(b, (z - s, y), 3, s - 1)
        if not last:
            self.send(b, (z - s, y), 3, s, (z + 1, y))
        if not last:
            self.arrived(b, (z + s, y), 4, s - 1)
            if s + 1 < HALF:
                self.send(b, (z + s, y), 4, s, (z - 1, y))
        self.spread(s)
        if not last:
            self.spread(NZ - s)
        for d in (0, 1, 3, 2):
            if not last or d == 0:
                self.arrived(a, (z - s, y - d), 1, 4 * (s - 1) + d)
                if s + 1 < HALF or s + 1 == HALF and d == 0:
                    self.send(a, (z - s, y - d), 1, 4 * s + d, (z + 1, y))
            if not last or d > 0:
                self.arrived(a, (z + s, y - d), 2, 4 * (s - 1) + d)
                if s + 1 < HALF or s + 1 == HALF and d > 0:
                    self.send(a, (z + s, y - d), 2, 4 * s + d, (z - 1, y))
            between()

    def along_y(self, k):
        z, y = self.z, self.y
        turn = 1 - 2 * (k % 2)
        both = self.b.at[pl.ds(0, 2 * self.rows[id(self.b)])]
        pltpu.make_async_remote_copy(
            src_ref=both, dst_ref=both, send_sem=self.s[id(self.b)].at[0], recv_sem=self.r[5].at[2 * k],
            device_id={"sp": rem(z + 1, NZ) * NY + y}, device_id_type=MESH,
        ).wait_recv()
        if k != HALF:
            self.send(self.b, (z - k, y - turn), 5, 2 * k + 1, (z, y + turn))

    def along_y_last(self, k):
        self.arrived(self.b, (self.z - k, self.y + 2), 5, 2 * k + 1)

    def finish(self):
        for ref in (self.a, self.b):
            everything = ref.at[pl.ds(0, self.sent[id(ref)] * self.rows[id(ref)])]
            pltpu.make_async_remote_copy(
                src_ref=everything, dst_ref=everything, send_sem=self.s[id(ref)].at[0], recv_sem=self.r[0].at[0],
                device_id={"sp": rem(self.z + 1, NZ) * NY + self.y}, device_id_type=MESH,
            ).wait_send()

    @staticmethod
    def semaphores():
        counts = [1, 1, 3, 4 * HALF, 4 * HALF, HALF, HALF, 2 * NZ]
        return [pltpu.SemaphoreType.DMA((n,)) for n in counts]


N_SEMS = 8


def groups_of(step):
    if step == 0:
        return [0]
    if step < HALF:
        return [step, NZ - step]
    return [step] if step == HALF else []


def expm1_negated(v):
    series = jnp.ones_like(v)
    for n in range(9, 1, -1):
        series = 1.0 + series * v * (1.0 / n)
    return jnp.where(v > -0.5, -v * series, 1.0 - jnp.exp(v))


def softplus_negated(b):
    e = jnp.exp(-jnp.abs(b))
    w = e / (2.0 + e)
    q = w * w
    series = jnp.full_like(w, 1.0 / 15.0)
    for n in (13, 11, 9, 7, 5, 3, 1):
        series = 1.0 / n + series * q
    return jnp.maximum(-b, 0.0) + 2.0 * w * series


NT_DIMS = (((1,), (1,)), ((), ()))
TN_DIMS = (((0,), (0,)), ((), ()))
SEGS = 8


def whole_kernel(*refs):
    n_in = 16
    given, out, scratch = refs[:n_in], refs[n_in], refs[n_in + 1 :]
    held, in_sem, scratch = scratch[:n_in], scratch[n_in], scratch[n_in + 1 :]
    loads = [pltpu.make_async_copy(g, h, in_sem.at[n]) for n, (g, h) in enumerate(zip(given, held))]
    for load in loads:
        load.start()
    (tokens, gain, wv_own, wg_own, ri_own, rg_own, oc_own, or_own, taps, bias, cgain, staps, dmap, imap, base,
     jump_t) = held
    (nt, wa, wb, acc_a, acc_b, oc, packed, orr, ext_c, ext_r, filt, md, mi, stats, dbuf, ibuf, gbuf, co, ro,
     jump, cy, cz, pc, ps, pr, s2, sp_buf, sm_buf, two, from_m, from_p) = scratch[:31]
    scratch = scratch[31:]
    sems_in, sems_out = scratch[:N_SEMS], scratch[N_SEMS : 2 * N_SEMS]
    (tok_s, tok_r, edge_s, edge_r, stat_s, stat_r, cy_s, cy_r, cz_s, cz_r, pr_s, pr_r, x_s, x_r) = scratch[2 * N_SEMS :]
    sp, tp = lax.axis_index("sp"), lax.axis_index("tp")
    z, y, x, c = sp // NY, sp % NY, tp // NC, tp % NC
    rows = wv_own.shape[0]
    n_tok, width = tokens.shape
    length = acc_a.shape[0]
    cw, rw = wv_own.shape[1], ri_own.shape[1]
    f32, bf16 = jnp.float32, jnp.bfloat16

    barrier = pltpu.get_barrier_semaphore()
    for dz, dy in ((1, 0), (-1, 0), (0, 1), (0, 2), (0, 3)):
        pl.semaphore_signal(
            barrier, inc=1, device_id={"sp": rem(z + dz, NZ) * NY + rem(y + dy, NY)}, device_id_type=MESH
        )
    for d in (1, -1):
        pl.semaphore_signal(barrier, inc=1, device_id={"sp": rem(sp + d, NZ * NY)}, device_id_type=MESH)
    for d in range(1, NX * NC):
        pl.semaphore_signal(barrier, inc=1, device_id={"tp": rem(tp + d, NX * NC)}, device_id_type=MESH)

    for load in loads:
        load.wait()
    own = pl.ds(pl.multiple_of(sp * rows, rows), rows)
    extra = wa.shape[1] - rw
    wa[own, :] = jnp.concatenate([ri_own[...], rg_own[:, :extra]], axis=1)
    wb[own, :cw] = wv_own[...]
    wb[own, cw : 2 * cw] = wg_own[...]
    wb[own, 2 * cw :] = rg_own[:, extra:]
    oc[own] = oc_own[...]
    p_rows, h_rows = rows + rows // 2, rows // 2
    p_at = pl.multiple_of(sp * p_rows, h_rows)
    packed[pl.ds(p_at, rows)] = or_own[:, :128]
    packed[pl.ds(p_at + rows, h_rows)] = jnp.concatenate([or_own[:h_rows, 128:], or_own[h_rows:, 128:]], axis=1)

    def unpack(k):
        for n in range(NY):
            chunk = rem(z - k, NZ) * NY + n
            src = pl.multiple_of(chunk * p_rows, h_rows)
            dst = pl.multiple_of(chunk * rows, rows)
            orr[pl.ds(dst, rows), :128] = packed[pl.ds(src, rows)]
            pair = packed[pl.ds(src + rows, h_rows)]
            orr[pl.ds(dst, h_rows), 128:rw] = pair[:, : rw - 128]
            orr[pl.ds(dst + h_rows, h_rows), 128:rw] = pair[:, rw - 128 :]

    pl.semaphore_wait(barrier, 7 + NX * NC - 1)

    g_in = Gather(wa, wb, (rows, rows), sems_in, (z, y))
    g_out = Gather(oc, packed, (rows, rows + rows // 2), sems_out, (z, y))
    g_in.start_z()
    g_in.start_y()
    g_in.spread(0)
    g_out.start_z()

    def tok_rows(xx, cc):
        return pl.ds(pl.multiple_of((rem(xx, NX) * NC + rem(cc, NC)) * n_tok, 16), n_tok)

    def tok_at(xx, cc, lanes=None):
        r = tok_rows(xx, cc)
        return nt.at[r] if lanes is None else nt.at[r, lanes]

    def tok_copy(block, index, xx, cc):
        return pltpu.make_async_remote_copy(
            src_ref=block, dst_ref=block, send_sem=tok_s.at[0], recv_sem=tok_r.at[index],
            device_id={"tp": rem(xx, NX) * NC + rem(cc, NC)}, device_id_type=MESH,
        )

    def tok_send(*args):
        tok_copy(*args).start()

    lo, hi = pl.ds(0, width // 2), pl.ds(width // 2, width // 2)

    widened = tokens[...].astype(f32)
    inverse = lax.rsqrt(jnp.mean(widened * widened, axis=-1, keepdims=True) + 1e-06)
    tok_at(x, c)[...] = (widened * inverse * gain[...]).astype(bf16)
    tok_send(tok_at(x, c), 0, x + 1, c)
    tok_send(tok_at(x, c), 1, x - 1, c)
    tok_send(tok_at(x, c), 4, x, c + 1)
    g_in.from_y()
    g_out.start_y()
    acc_a[...] = jnp.zeros_like(acc_a)
    acc_b[...] = jnp.zeros_like(acc_b)
    cy[...] = jnp.zeros_like(cy)
    cz[...] = jnp.zeros_like(cz)
    head = dmap.shape[1]
    for m, given in ((md, dmap), (mi, imap)):
        m[...] = jnp.zeros_like(m)
        for h in range(dmap.shape[0]):
            m[h * head : (h + 1) * head, h * head : (h + 1) * head] = given[h]
    jump[...] = jnp.transpose(jump_t[...])

    def tokens_forward():
        tok_copy(tok_at(x - 1, c), 0, x + 1, c).wait_recv()
        tok_send(tok_at(x - 1, c, lo), 2, x + 1, c)
        tok_send(tok_at(x - 1, c), 5, x, c + 1)
        tok_copy(tok_at(x + 1, c), 1, x + 1, c).wait_recv()
        tok_send(tok_at(x + 1, c, hi), 3, x - 1, c)
        tok_send(tok_at(x + 1, c), 6, x, c + 1)

    def tokens_relay():
        tok_copy(tok_at(x + 2, c, lo), 2, x + 1, c).wait_recv()
        tok_send(tok_at(x + 2, c, lo), 7, x, c + 1)
        tok_copy(tok_at(x + 2, c, hi), 3, x + 1, c).wait_recv()
        tok_send(tok_at(x + 2, c, hi), 8, x, c + 1)

    def tokens_last():
        tok_copy(tok_at(x, c + 1), 4, x + 1, c).wait_recv()
        tok_copy(tok_at(x - 1, c + 1), 5, x + 1, c).wait_recv()
        tok_copy(tok_at(x + 1, c + 1), 6, x + 1, c).wait_recv()
        tok_copy(tok_at(x + 2, c + 1, lo), 7, x + 1, c).wait_recv()
        tok_copy(tok_at(x + 2, c + 1, hi), 8, x + 1, c).wait_recv()

    def multiply(acc, w, first, last):
        def body(j, carry):
            s = (j + 1) // 2
            zz = rem(z + jnp.where(j % 2 == 1, -s, s), NZ)
            cols = pl.ds(pl.multiple_of(zz * (NY * rows), NY * rows), NY * rows)
            acc[...] += jnp.dot(nt[:, cols], w[cols, :], preferred_element_type=f32)
            return carry

        lax.fori_loop(first, last, body, 0)

    a_part = lambda first, last: (lambda: multiply(acc_a, wa, first, last))
    b_part = lambda first, last: (lambda: multiply(acc_b, wb, first, last))
    work = {
        6: [a_part(0, 2), a_part(2, 4), a_part(4, 6), a_part(6, 8)],
        7: [a_part(8, 10), a_part(10, 12), b_part(0, 2), b_part(2, 4)],
        8: [b_part(4, 6), b_part(6, 8), b_part(8, 10), a_part(12, 15)],
    }

    def out_step(s):
        if s == 0:
            g_out.spread(0)
            g_out.from_y()
        elif s <= HALF:
            g_out.along_z(s)
        if s >= 1:
            for k in groups_of(s - 1):
                g_out.along_y(k)
        if s >= 2:
            for k in groups_of(s - 2):
                g_out.along_y_last(k)
                unpack(k)

    lag = 3

    def at_step(step):
        todo = list(work.get(step, []))
        g_in.along_z(step, lambda: todo and todo.pop(0)())
        if step == HALF:
            a_part(NZ - 1, NZ)()
            start_recurrence()
        for k in groups_of(step - 1):
            g_in.along_y(k)
        if step >= lag:
            out_step(step - lag)
        if step >= 2:
            for k in groups_of(step - 2):
                g_in.along_y_last(k)
        if step == 2:
            tokens_forward()
        if step == 4:
            tokens_relay()
        if step == 5:
            tokens_last()

    c_pad, r_pad = ext_c.shape[0] - length, ext_r.shape[0] - length

    def edge_copy(ref, pad, index):
        return pltpu.make_async_remote_copy(
            src_ref=ref.at[pl.ds(length, pad)], dst_ref=ref.at[pl.ds(0, pad)],
            send_sem=edge_s.at[index], recv_sem=edge_r.at[index],
            device_id={"sp": rem(sp + 1, NZ * NY)}, device_id_type=MESH,
        )

    edges = [edge_copy(ext_r, r_pad, 0), edge_copy(ext_c, c_pad, 1)]

    def take_edge(index, ref, pad):
        edges[index].wait_recv()
        ref[:pad, :] = jnp.where(sp > 0, ref[:pad, :], 0.0)

    def start_recurrence():
        ext_r[r_pad:, :] = acc_a[:, :rw].astype(bf16).astype(f32)
        edges[0].start()

    for step in range(1, HALF + 1):
        at_step(step)

    n_short = staps.shape[0]
    short = staps[...].astype(f32)
    rate = -RATE_SCALE * softplus_negated(base[...])
    tile = 128
    n_tiles = dbuf.shape[0]

    def gates(first, count):
        smoothed = jnp.zeros((count, rw), f32)
        for k in range(n_short):
            at = r_pad - (n_short - 1) + k + first
            smoothed = smoothed + short[k : k + 1, :] * ext_r[at : at + count, :]
        rounded = smoothed.astype(bf16)
        retain = jax.nn.sigmoid(jnp.dot(rounded, md[...], preferred_element_type=f32))
        admit = jax.nn.sigmoid(jnp.dot(rounded, mi[...], preferred_element_type=f32))
        log_decay = rate * retain + jump[first : first + count, :]
        decay = jnp.exp(log_decay)
        inflow = jnp.sqrt(expm1_negated(2.0 * log_decay)) * admit * rounded.astype(f32)
        for n in range(n_tiles):
            used = min(tile, rw - n * tile)
            dbuf[n, first : first + count, :used] = decay[:, n * tile : n * tile + used]
            ibuf[n, first : first + count, :used] = inflow[:, n * tile : n * tile + used]

    early = 16
    gates(early, length - early)
    b_part(10, 13)()
    take_edge(0, ext_r, r_pad)
    gates(0, early)
    seg = length // SEGS

    def scan_step(j, carry):
        new = []
        for n, (p, s) in enumerate(carry):
            at = (n, pl.ds(j, SEGS, stride=seg), slice(None))
            d, i = dbuf[at], ibuf[at]
            p, s = d * p, d * s + i
            dbuf[at] = p
            ibuf[at] = s
            new.append((p, s))
        return tuple(new)

    start = tuple((jnp.ones((SEGS, tile), f32), jnp.zeros((SEGS, tile), f32)) for _ in range(n_tiles))
    ends = lax.fori_loop(0, seg, scan_step, start)
    p_all = jnp.concatenate([e[0] for e in ends], axis=1)
    s_all = jnp.concatenate([e[1] for e in ends], axis=1)
    half = cy.shape[2] // 2
    p_run, s_run = jnp.ones((1, half), f32), jnp.zeros((1, half), f32)
    before = []
    for g in range(SEGS):
        before.append((p_run, s_run))
        p_g, s_g = p_all[g : g + 1, :], s_all[g : g + 1, :]
        p_run, s_run = p_run * p_g, p_g * s_run + s_g

    def carry_copy(buf, slot, send, recv, to):
        return pltpu.make_async_remote_copy(
            src_ref=buf.at[slot], dst_ref=buf.at[slot], send_sem=send.at[0], recv_sem=recv.at[0],
            device_id={"sp": rem(to[0], NZ) * NY + rem(to[1], NY)}, device_id_type=MESH,
        )

    cy[y, :, :half] = p_run
    cy[y, :, half:] = s_run
    for d in range(1, NY):
        carry_copy(cy, pl.ds(y, 1), cy_s, cy_r, (z, y + d)).start()
    out_step(HALF + 1 - lag)
    for k in groups_of(HALF):
        g_in.along_y(k)
    for k in groups_of(HALF - 1) + groups_of(HALF):
        g_in.along_y_last(k)
    b_part(13, NZ)()
    conv_val = acc_b[:, :cw].astype(bf16).astype(f32)
    conv_gate = acc_b[:, cw : 2 * cw].astype(bf16).astype(f32)
    ext_c[c_pad:, :] = (conv_val * jax.nn.sigmoid(conv_gate)).astype(bf16).astype(f32)
    edges[1].start()
    gate = jnp.concatenate([acc_a[:, rw:], acc_b[:, 2 * cw :]], axis=1).astype(bf16).astype(f32)
    gbuf[...] = 0.5 * gate * (1.0 + jnp.tanh(0.7978845608028654 * (gate + 0.044715 * gate * gate * gate)))
    carry_copy(cy, pl.ds(0, NY - 1), cy_s, cy_r, (z, y + 1)).wait_recv()
    p_run, s_run = jnp.ones((1, half), f32), jnp.zeros((1, half), f32)
    p_mine, s_mine = p_run, s_run
    for n in range(NY):
        p_mine = jnp.where(y == n, p_run, p_mine)
        s_mine = jnp.where(y == n, s_run, s_mine)
        p_n, s_n = cy[n, :, :half], cy[n, :, half:]
        p_run, s_run = p_run * p_n, p_n * s_run + s_n
    cz[z, :, :half] = p_run
    cz[z, :, half:] = s_run
    for d in range(1, NZ):
        carry_copy(cz, pl.ds(z, 1), cz_s, cz_r, (z + d, y)).start()
    out_step(HALF + 2 - lag)
    n_taps = taps.shape[0]
    wide = taps[...].astype(f32)
    tap_rows = 32

    def filter_rows(first):
        total = jnp.broadcast_to(bias[...], (tap_rows, cw))
        for k in range(n_taps):
            at = first + c_pad - (n_taps - 1) + k
            total = total + wide[k : k + 1, :] * ext_c[at : at + tap_rows, :]
        filt[first : first + tap_rows, :] = total

    for i in range(1, length // tap_rows):
        filter_rows(i * tap_rows)
    take_edge(1, ext_c, c_pad)
    filter_rows(0)
    filtered = filt[...]
    row_id = lax.broadcasted_iota(jnp.int32, (8, cw), 0)
    first_half = jnp.where(row_id < 4, 1.0, 0.0)
    exact = lax.Precision.HIGHEST
    stats[tp] = lax.dot_general(
        first_half, filtered, NT_DIMS, precision=exact, preferred_element_type=f32
    ) + lax.dot_general(
        1.0 - first_half, filtered * filtered, NT_DIMS, precision=exact, preferred_element_type=f32
    )

    def stat_copy(d):
        return pltpu.make_async_remote_copy(
            src_ref=stats.at[tp], dst_ref=stats.at[tp], send_sem=stat_s.at[0], recv_sem=stat_r.at[0],
            device_id={"tp": rem(tp + d, NX * NC)}, device_id_type=MESH,
        )

    stats_of_others = pltpu.make_async_remote_copy(
        src_ref=stats.at[pl.ds(0, NX * NC - 1)], dst_ref=stats.at[pl.ds(0, NX * NC - 1)],
        send_sem=stat_s.at[0], recv_sem=stat_r.at[0],
        device_id={"tp": rem(tp + 1, NX * NC)}, device_id_type=MESH,
    )

    for d in range(1, NX * NC):
        stat_copy(d).start()

    out_step(HALF + 3 - lag)
    stats_of_others.wait_recv()
    totals = stats[0]
    for n in range(1, NX * NC):
        totals = totals + stats[n]
    scale = 1.0 / CONV_WIDTH
    row_id = lax.broadcasted_iota(jnp.int32, (8, cw), 0)
    mean = lax.dot_general(
        totals * scale, jnp.where(row_id == 0, 1.0, 0.0), TN_DIMS, precision=exact, preferred_element_type=f32
    )
    square = lax.dot_general(
        totals * scale, jnp.where(row_id == 4, 1.0, 0.0), TN_DIMS, precision=exact, preferred_element_type=f32
    )
    spread = jnp.maximum(square - mean * mean, 0.0)
    scaled = (filt[...] - mean) * lax.rsqrt(spread + 1e-05) * cgain[...]
    co[...] = (scaled * jax.nn.sigmoid(scaled)).astype(bf16)
    out_step(HALF + 4 - lag)
    out_step(HALF + 5 - lag)
    for s in range(max(HALF + 6 - lag, 0), HALF + 3):
        out_step(s)
    carry_copy(cz, pl.ds(0, NZ - 1), cz_s, cz_r, (z + 1, y)).wait_recv()
    entering = jnp.zeros((1, half), f32)
    for n in range(NZ):
        entering = jnp.where(n < z, cz[n, :, :half] * entering + cz[n, :, half:], entering)
    entering = p_mine * entering + s_mine
    for g, (p_g, s_g) in enumerate(before):
        part = slice(g * seg, (g + 1) * seg)
        at_start = p_g * entering + s_g
        for n in range(n_tiles):
            used = min(tile, rw - n * tile)
            lanes = slice(n * tile, n * tile + used)
            state = ibuf[n, part, :used] + dbuf[n, part, :used] * at_start[:, lanes]
            ro[part, lanes] = (gbuf[part, lanes] * state).astype(bf16)

    def chip_rows(xx, cc):
        return pl.ds(pl.multiple_of((rem(xx, NX) * NC + rem(cc, NC)) * n_tok, n_tok), n_tok)

    block = 512

    def out_part(j, carry):
        cols = pl.ds(pl.multiple_of(j * block, block), block)
        pc[:, cols] = lax.dot_general(
            co[...], oc[cols, :], NT_DIMS, preferred_element_type=f32
        ) + lax.dot_general(ro[...], orr[cols, :rw], NT_DIMS, preferred_element_type=f32)
        for d in range(NX):
            ps[d, :, cols] = pc[chip_rows(x + d, c + 1), cols].astype(bf16)
        return carry

    quarter = width // 4

    def lanes_of(q):
        return slice(q * quarter, (q + 1) * quarter)

    def pair_copy(d, q):
        lanes = lanes_of(q)
        return pltpu.make_async_remote_copy(
            src_ref=ps.at[d, :, lanes], dst_ref=pr.at[d, :, lanes],
            send_sem=pr_s.at[0], recv_sem=pr_r.at[4 * d + q],
            device_id={"tp": x * NC + rem(c + 1, NC)}, device_id_type=MESH,
        )

    def project(q):
        n_blocks = quarter // block
        lax.fori_loop(q * n_blocks, (q + 1) * n_blocks, out_part, 0)
        for d in (2, 1, 3, 0):
            pair_copy(d, q).start()

    def x_copy(src, dst, index, q, xx):
        return pltpu.make_async_remote_copy(
            src_ref=src.at[:, lanes_of(q)], dst_ref=dst.at[:, lanes_of(q)],
            send_sem=x_s.at[index // 4], recv_sem=x_r.at[index],
            device_id={"tp": rem(xx, NX) * NC + c}, device_id_type=MESH,
        )

    def chip_sum(d, q):
        pair_copy(d, q).wait_recv()
        return pc[chip_rows(x + d, c), lanes_of(q)] + pr[d, :, lanes_of(q)].astype(f32)

    far = [x_copy(s2, two, q, q, x + 1 if q < 2 else x - 1) for q in range(4)]
    up = [x_copy(sp_buf, from_m, 4 + q, q, x + 1) for q in range(4)]
    down = [x_copy(sm_buf, from_p, 8 + q, q, x - 1) for q in range(4)]

    def send_far(q):
        s2[:, lanes_of(q)] = chip_sum(2, q).astype(bf16)
        far[q].start()

    def send_near(d, q):
        buf, copies = (sp_buf, up) if d == 1 else (sm_buf, down)
        total = chip_sum(d, q)
        if (q < 2) == (d == 1):
            far[q].wait_recv()
            total = total + two[:, lanes_of(q)].astype(f32)
        buf[:, lanes_of(q)] = total.astype(bf16)
        copies[q].start()

    project(0)
    project(2)
    send_far(0)
    send_far(2)
    project(1)
    project(3)
    send_near(3, 0)
    send_near(1, 2)
    send_far(1)
    send_far(3)
    send_near(3, 1)
    send_near(1, 3)
    send_near(1, 0)
    send_near(3, 2)
    send_near(1, 1)
    send_near(3, 3)
    mine = chip_rows(x, c)
    for q in range(4):
        pc[mine, lanes_of(q)] = chip_sum(0, q)
    for q in (0, 2, 1, 3):
        at = lanes_of(q)
        up[q].wait_recv()
        down[q].wait_recv()
        out[:, at] = (pc[mine, at] + (from_m[:, at].astype(f32) + from_p[:, at].astype(f32))).astype(bf16)

    g_in.finish()
    g_out.finish()
    tok_copy(nt.at[pl.ds(0, 7 * n_tok)], 0, x + 1, c).wait_send()
    for e in edges:
        e.wait_send()
    stats_of_others.wait_send()
    carry_copy(cy, pl.ds(0, NY - 1), cy_s, cy_r, (z, y + 1)).wait_send()
    carry_copy(cz, pl.ds(0, NZ - 1), cz_s, cz_r, (z + 1, y)).wait_send()
    pltpu.make_async_remote_copy(
        src_ref=ps, dst_ref=pr, send_sem=pr_s.at[0], recv_sem=pr_r.at[0],
        device_id={"tp": x * NC + rem(c + 1, NC)}, device_id_type=MESH,
    ).wait_send()
    for n, buf in enumerate((s2, sp_buf, sm_buf)):
        pltpu.make_async_remote_copy(
            src_ref=buf, dst_ref=two, send_sem=x_s.at[n], recv_sem=x_r.at[0],
            device_id={"tp": rem(x + 1, NX) * NC + c}, device_id_type=MESH,
        ).wait_send()


def shards(
    tokens, norm_gain, conv_val_w, conv_gate_w, rec_gate_w, rec_in_w, conv_taps, conv_bias, conv_gain,
    short_taps, decay_map, input_map, decay_base, decay_jump, out_conv_w, out_rec_w,
):
    cw, rw = conv_val_w.shape[1], rec_in_w.shape[1]
    n_tok, width = tokens.shape
    length = n_tok * NX * NC
    wide = rw + -rw % 128
    f32, bf16 = jnp.float32, jnp.bfloat16
    vmem = pl.BlockSpec(memory_space=pltpu.VMEM)
    V, S = pltpu.VMEM, pltpu.SemaphoreType.DMA
    given = (
        tokens,
        norm_gain[None, :],
        conv_val_w,
        conv_gate_w,
        rec_in_w,
        rec_gate_w,
        out_conv_w.T,
        out_rec_w.T,
        conv_taps,
        conv_bias[None, :],
        conv_gain[None, :],
        short_taps,
        decay_map,
        input_map,
        decay_base[None, :],
        decay_jump.T,
    )
    return pl.pallas_call(
        whole_kernel,
        out_shape=pltpu.VMEM((n_tok, width), bf16),
        in_specs=[pl.BlockSpec(memory_space=pltpu.HBM)] * 16,
        out_specs=vmem,
        scratch_shapes=[
            *(V(g.shape, g.dtype) for g in given),
            S((16,)),
            V((length, width), bf16),
            V((width, 2 * cw), bf16),
            V((width, 2 * rw), bf16),
            V((length, 2 * cw), f32),
            V((length, 2 * rw), f32),
            V((width, cw), bf16),
            V((width * 3 // 2, 128), bf16),
            V((width, wide), bf16),
            V((length + 32, cw), f32),
            V((length + 8, rw), f32),
            V((length, cw), f32),
            V((rw, rw), bf16),
            V((rw, rw), bf16),
            V((NX * NC, 8, length), f32),
            V((wide // 128, length, 128), f32),
            V((wide // 128, length, 128), f32),
            V((length, rw), f32),
            V((length, cw), bf16),
            V((length, rw), bf16),
            V((length, rw), f32),
            V((NY, 1, 2 * wide), f32),
            V((NZ, 1, 2 * wide), f32),
            V((length, width), f32),
            V((NX, n_tok, width), bf16),
            V((NX, n_tok, width), bf16),
            V((n_tok, width), bf16),
            V((n_tok, width), bf16),
            V((n_tok, width), bf16),
            V((n_tok, width), bf16),
            V((n_tok, width), bf16),
            V((n_tok, width), bf16),
            *Gather.semaphores(),
            *Gather.semaphores(),
            S((1,)), S((9,)), S((2,)), S((2,)), S((1,)), S((1,)), S((1,)), S((1,)),
            S((1,)), S((1,)), S((1,)), S((4 * NX,)), S((3,)), S((12,)),
        ],
        compiler_params=pltpu.CompilerParams(
            collective_id=0, has_side_effects=True, vmem_limit_bytes=66_640_000
        ),
    )(*given)


def solution(mesh):
    in_specs = (
        P(("sp", "tp"), None), P(), P("sp", "tp"), P("sp", "tp"), P("sp", "tp"), P("sp", "tp"),
        P(None, "tp"), P("tp"), P("tp"), P(None, "tp"), P("tp", None, None), P("tp", None, None),
        P("tp"), P("sp", "tp"), P("tp", "sp"), P("tp", "sp"),
    )
    return jax.shard_map(
        shards, mesh=mesh, in_specs=in_specs, out_specs=P(("sp", "tp"), None), check_vma=False
    )
```

```python
import jax
import jax.numpy as jnp
from jax import lax
from jax.experimental import pallas as pl
from jax.experimental.pallas import tpu as pltpu
from jax.sharding import PartitionSpec as P

MESH = pl.DeviceIdType.MESH
CONV_WIDTH = 1024
RATE_SCALE = 8.0
NZ, NY, NX, NC = 16, 4, 4, 2
HALF = NZ // 2


def rem(a, n):
    return lax.rem(a + 4 * n, n)


class Gather:
    def __init__(self, a, b, rows, sems, pos):
        self.a, self.b = a, b
        self.rows = {id(a): rows[0], id(b): rows[1]}
        self.s, self.r = {id(a): sems[0], id(b): sems[1]}, sems[2:]
        self.z, self.y = pos
        self.sent = {id(a): 0, id(b): 0}

    def at(self, ref, z, y):
        rows = self.rows[id(ref)]
        return ref.at[pl.ds(pl.multiple_of((rem(z, NZ) * NY + rem(y, NY)) * rows, rows), rows)]

    def copy(self, ref, chunk, kind, index, to):
        block = self.at(ref, *chunk)
        return pltpu.make_async_remote_copy(
            src_ref=block,
            dst_ref=block,
            send_sem=self.s[id(ref)].at[0],
            recv_sem=self.r[kind].at[index],
            device_id={"sp": rem(to[0], NZ) * NY + rem(to[1], NY)},
            device_id_type=MESH,
        )

    def send(self, *args):
        self.copy(*args).start()
        self.sent[id(args[0])] += 1

    def arrived(self, ref, chunk, kind, index):
        self.copy(ref, chunk, kind, index, (self.z + 1, self.y)).wait_recv()

    def start_y(self):
        z, y, a = self.z, self.y, self.a
        for d in (1, 3, 2):
            self.send(a, (z, y), 0, d - 1, (z, y + d))

    def start_z(self):
        z, y = self.z, self.y
        for ref, up in ((self.b, 3), (self.a, 1)):
            self.send(ref, (z, y), up, 0, (z + 1, y))
            self.send(ref, (z, y), up + 1, 0, (z - 1, y))

    def from_y(self):
        z, y, a = self.z, self.y, self.a
        for d in (1, 3, 2):
            self.arrived(a, (z, y - d), 0, d - 1)
            self.send(a, (z, y - d), 1, d, (z + 1, y))
            self.send(a, (z, y - d), 2, d, (z - 1, y))

    def spread(self, k):
        z, y = self.z, self.y
        self.send(self.b, (z - k, y), 5, 2 * k, (z, y + 1))
        self.send(self.b, (z - k, y), 5, 2 * k, (z, y - 1))
        if k == HALF:
            self.send(self.b, (z - k, y), 5, 2 * k + 1, (z, y + 2))

    def along_z(self, s, between=lambda: None):
        z, y, a, b = self.z, self.y, self.a, self.b
        last = s == HALF
        self.arrived(b, (z - s, y), 3, s - 1)
        if not last:
            self.send(b, (z - s, y), 3, s, (z + 1, y))
        if not last:
            self.arrived(b, (z + s, y), 4, s - 1)
            if s + 1 < HALF:
                self.send(b, (z + s, y), 4, s, (z - 1, y))
        self.spread(s)
        if not last:
            self.spread(NZ - s)
        for d in (0, 1, 3, 2):
            if not last or d == 0:
                self.arrived(a, (z - s, y - d), 1, 4 * (s - 1) + d)
                if s + 1 < HALF or s + 1 == HALF and d == 0:
                    self.send(a, (z - s, y - d), 1, 4 * s + d, (z + 1, y))
            if not last or d > 0:
                self.arrived(a, (z + s, y - d), 2, 4 * (s - 1) + d)
                if s + 1 < HALF or s + 1 == HALF and d > 0:
                    self.send(a, (z + s, y - d), 2, 4 * s + d, (z - 1, y))
            between()

    def along_y(self, k):
        z, y = self.z, self.y
        turn = 1 - 2 * (k % 2)
        both = self.b.at[pl.ds(0, 2 * self.rows[id(self.b)])]
        pltpu.make_async_remote_copy(
            src_ref=both, dst_ref=both, send_sem=self.s[id(self.b)].at[0], recv_sem=self.r[5].at[2 * k],
            device_id={"sp": rem(z + 1, NZ) * NY + y}, device_id_type=MESH,
        ).wait_recv()
        if k != HALF:
            self.send(self.b, (z - k, y - turn), 5, 2 * k + 1, (z, y + turn))

    def along_y_last(self, k):
        self.arrived(self.b, (self.z - k, self.y + 2), 5, 2 * k + 1)

    def finish(self):
        for ref in (self.a, self.b):
            everything = ref.at[pl.ds(0, self.sent[id(ref)] * self.rows[id(ref)])]
            pltpu.make_async_remote_copy(
                src_ref=everything, dst_ref=everything, send_sem=self.s[id(ref)].at[0], recv_sem=self.r[0].at[0],
                device_id={"sp": rem(self.z + 1, NZ) * NY + self.y}, device_id_type=MESH,
            ).wait_send()

    @staticmethod
    def semaphores():
        counts = [1, 1, 3, 4 * HALF, 4 * HALF, HALF, HALF, 2 * NZ]
        return [pltpu.SemaphoreType.DMA((n,)) for n in counts]


N_SEMS = 8


def groups_of(step):
    if step == 0:
        return [0]
    if step < HALF:
        return [step, NZ - step]
    return [step] if step == HALF else []


def expm1_negated(v):
    series = jnp.ones_like(v)
    for n in range(9, 1, -1):
        series = 1.0 + series * v * (1.0 / n)
    return jnp.where(v > -0.5, -v * series, 1.0 - jnp.exp(v))


def softplus_negated(b):
    e = jnp.exp(-jnp.abs(b))
    w = e / (2.0 + e)
    q = w * w
    series = jnp.full_like(w, 1.0 / 15.0)
    for n in (13, 11, 9, 7, 5, 3, 1):
        series = 1.0 / n + series * q
    return jnp.maximum(-b, 0.0) + 2.0 * w * series


NT_DIMS = (((1,), (1,)), ((), ()))
TN_DIMS = (((0,), (0,)), ((), ()))
SEGS = 8


def whole_kernel(*refs):
    n_in = 16
    given, out, scratch = refs[:n_in], refs[n_in], refs[n_in + 1 :]
    held, in_sem, scratch = scratch[:n_in], scratch[n_in], scratch[n_in + 1 :]
    loads = [pltpu.make_async_copy(g, h, in_sem.at[n]) for n, (g, h) in enumerate(zip(given, held))]
    for load in loads:
        load.start()
    (tokens, gain, wv_own, wg_own, ri_own, rg_own, oc_own, or_own, taps, bias, cgain, staps, dmap, imap, base,
     jump_t) = held
    (nt, wa, wb, acc_a, acc_b, oc, packed, orr, ext_c, ext_r, filt, md, mi, stats, dbuf, ibuf, gbuf, co, ro,
     jump, cy, cz, pc, ps, pr, s2, sp_buf, sm_buf, two, from_m, from_p) = scratch[:31]
    scratch = scratch[31:]
    sems_in, sems_out = scratch[:N_SEMS], scratch[N_SEMS : 2 * N_SEMS]
    (tok_s, tok_r, edge_s, edge_r, stat_s, stat_r, cy_s, cy_r, cz_s, cz_r, pr_s, pr_r, x_s, x_r) = scratch[2 * N_SEMS :]
    sp, tp = lax.axis_index("sp"), lax.axis_index("tp")
    z, y, x, c = sp // NY, sp % NY, tp // NC, tp % NC
    rows = wv_own.shape[0]
    n_tok, width = tokens.shape
    length = acc_a.shape[0]
    cw, rw = wv_own.shape[1], ri_own.shape[1]
    f32, bf16 = jnp.float32, jnp.bfloat16

    barrier = pltpu.get_barrier_semaphore()
    for dz, dy in ((1, 0), (-1, 0), (0, 1), (0, 2), (0, 3)):
        pl.semaphore_signal(
            barrier, inc=1, device_id={"sp": rem(z + dz, NZ) * NY + rem(y + dy, NY)}, device_id_type=MESH
        )
    for d in (1, -1):
        pl.semaphore_signal(barrier, inc=1, device_id={"sp": rem(sp + d, NZ * NY)}, device_id_type=MESH)
    for d in range(1, NX * NC):
        pl.semaphore_signal(barrier, inc=1, device_id={"tp": rem(tp + d, NX * NC)}, device_id_type=MESH)

    for load in loads:
        load.wait()
    own = pl.ds(pl.multiple_of(sp * rows, rows), rows)
    extra = wa.shape[1] - rw
    wa[own, :] = jnp.concatenate([ri_own[...], rg_own[:, :extra]], axis=1)
    wb[own, :cw] = wv_own[...]
    wb[own, cw : 2 * cw] = wg_own[...]
    wb[own, 2 * cw :] = rg_own[:, extra:]
    oc[own] = oc_own[...]
    p_rows, h_rows = rows + rows // 2, rows // 2
    p_at = pl.multiple_of(sp * p_rows, h_rows)
    packed[pl.ds(p_at, rows)] = or_own[:, :128]
    packed[pl.ds(p_at + rows, h_rows)] = jnp.concatenate([or_own[:h_rows, 128:], or_own[h_rows:, 128:]], axis=1)

    def unpack(k):
        for n in range(NY):
            chunk = rem(z - k, NZ) * NY + n
            src = pl.multiple_of(chunk * p_rows, h_rows)
            dst = pl.multiple_of(chunk * rows, rows)
            orr[pl.ds(dst, rows), :128] = packed[pl.ds(src, rows)]
            pair = packed[pl.ds(src + rows, h_rows)]
            orr[pl.ds(dst, h_rows), 128:rw] = pair[:, : rw - 128]
            orr[pl.ds(dst + h_rows, h_rows), 128:rw] = pair[:, rw - 128 :]

    pl.semaphore_wait(barrier, 7 + NX * NC - 1)

    g_in = Gather(wa, wb, (rows, rows), sems_in, (z, y))
    g_out = Gather(oc, packed, (rows, rows + rows // 2), sems_out, (z, y))
    g_in.start_z()
    g_in.start_y()
    g_in.spread(0)
    g_out.start_z()

    def tok_rows(xx, cc):
        return pl.ds(pl.multiple_of((rem(xx, NX) * NC + rem(cc, NC)) * n_tok, 16), n_tok)

    def tok_at(xx, cc, lanes=None):
        r = tok_rows(xx, cc)
        return nt.at[r] if lanes is None else nt.at[r, lanes]

    def tok_copy(block, index, xx, cc):
        return pltpu.make_async_remote_copy(
            src_ref=block, dst_ref=block, send_sem=tok_s.at[0], recv_sem=tok_r.at[index],
            device_id={"tp": rem(xx, NX) * NC + rem(cc, NC)}, device_id_type=MESH,
        )

    def tok_send(*args):
        tok_copy(*args).start()

    lo, hi = pl.ds(0, width // 2), pl.ds(width // 2, width // 2)

    widened = tokens[...].astype(f32)
    inverse = lax.rsqrt(jnp.mean(widened * widened, axis=-1, keepdims=True) + 1e-06)
    tok_at(x, c)[...] = (widened * inverse * gain[...]).astype(bf16)
    tok_send(tok_at(x, c), 0, x + 1, c)
    tok_send(tok_at(x, c), 1, x - 1, c)
    tok_send(tok_at(x, c), 4, x, c + 1)
    g_in.from_y()
    g_out.start_y()
    acc_a[...] = jnp.zeros_like(acc_a)
    acc_b[...] = jnp.zeros_like(acc_b)
    cy[...] = jnp.zeros_like(cy)
    cz[...] = jnp.zeros_like(cz)
    head = dmap.shape[1]
    for m, given in ((md, dmap), (mi, imap)):
        m[...] = jnp.zeros_like(m)
        for h in range(dmap.shape[0]):
            m[h * head : (h + 1) * head, h * head : (h + 1) * head] = given[h]
    jump[...] = jnp.transpose(jump_t[...])

    def tokens_forward():
        tok_copy(tok_at(x - 1, c), 0, x + 1, c).wait_recv()
        tok_send(tok_at(x - 1, c, lo), 2, x + 1, c)
        tok_send(tok_at(x - 1, c), 5, x, c + 1)
        tok_copy(tok_at(x + 1, c), 1, x + 1, c).wait_recv()
        tok_send(tok_at(x + 1, c, hi), 3, x - 1, c)
        tok_send(tok_at(x + 1, c), 6, x, c + 1)

    def tokens_relay():
        tok_copy(tok_at(x + 2, c, lo), 2, x + 1, c).wait_recv()
        tok_send(tok_at(x + 2, c, lo), 7, x, c + 1)
        tok_copy(tok_at(x + 2, c, hi), 3, x + 1, c).wait_recv()
        tok_send(tok_at(x + 2, c, hi), 8, x, c + 1)

    def tokens_last():
        tok_copy(tok_at(x, c + 1), 4, x + 1, c).wait_recv()
        tok_copy(tok_at(x - 1, c + 1), 5, x + 1, c).wait_recv()
        tok_copy(tok_at(x + 1, c + 1), 6, x + 1, c).wait_recv()
        tok_copy(tok_at(x + 2, c + 1, lo), 7, x + 1, c).wait_recv()
        tok_copy(tok_at(x + 2, c + 1, hi), 8, x + 1, c).wait_recv()

    def multiply(acc, w, first, last):
        def body(j, carry):
            s = (j + 1) // 2
            zz = rem(z + jnp.where(j % 2 == 1, -s, s), NZ)
            cols = pl.ds(pl.multiple_of(zz * (NY * rows), NY * rows), NY * rows)
            acc[...] += jnp.dot(nt[:, cols], w[cols, :], preferred_element_type=f32)
            return carry

        lax.fori_loop(first, last, body, 0)

    a_part = lambda first, last: (lambda: multiply(acc_a, wa, first, last))
    b_part = lambda first, last: (lambda: multiply(acc_b, wb, first, last))
    work = {
        6: [a_part(0, 2), a_part(2, 4), a_part(4, 6), a_part(6, 8)],
        7: [a_part(8, 10), a_part(10, 12), b_part(0, 2), b_part(2, 4)],
        8: [b_part(4, 6), b_part(6, 8), b_part(8, 10), a_part(12, 15)],
    }

    def out_step(s):
        if s == 0:
            g_out.spread(0)
            g_out.from_y()
        elif s <= HALF:
            g_out.along_z(s)
        if s >= 1:
            for k in groups_of(s - 1):
                g_out.along_y(k)
        if s >= 2:
            for k in groups_of(s - 2):
                g_out.along_y_last(k)
                unpack(k)

    lag = 3

    def at_step(step):
        todo = list(work.get(step, []))
        g_in.along_z(step, lambda: todo and todo.pop(0)())
        if step == HALF:
            a_part(NZ - 1, NZ)()
            start_recurrence()
        for k in groups_of(step - 1):
            g_in.along_y(k)
        if step >= lag:
            out_step(step - lag)
        if step >= 2:
            for k in groups_of(step - 2):
                g_in.along_y_last(k)
        if step == 2:
            tokens_forward()
        if step == 4:
            tokens_relay()
        if step == 5:
            tokens_last()

    c_pad, r_pad = ext_c.shape[0] - length, ext_r.shape[0] - length

    def edge_copy(ref, pad, index):
        return pltpu.make_async_remote_copy(
            src_ref=ref.at[pl.ds(length, pad)], dst_ref=ref.at[pl.ds(0, pad)],
            send_sem=edge_s.at[index], recv_sem=edge_r.at[index],
            device_id={"sp": rem(sp + 1, NZ * NY)}, device_id_type=MESH,
        )

    edges = [edge_copy(ext_r, r_pad, 0), edge_copy(ext_c, c_pad, 1)]

    def take_edge(index, ref, pad):
        edges[index].wait_recv()
        ref[:pad, :] = jnp.where(sp > 0, ref[:pad, :], 0.0)

    def start_recurrence():
        ext_r[r_pad:, :] = acc_a[:, :rw].astype(bf16).astype(f32)
        edges[0].start()

    for step in range(1, HALF + 1):
        at_step(step)

    n_short = staps.shape[0]
    short = staps[...].astype(f32)
    rate = -RATE_SCALE * softplus_negated(base[...])
    tile = 128
    n_tiles = dbuf.shape[0]

    def gates(first, count):
        smoothed = jnp.zeros((count, rw), f32)
        for k in range(n_short):
            at = r_pad - (n_short - 1) + k + first
            smoothed = smoothed + short[k : k + 1, :] * ext_r[at : at + count, :]
        rounded = smoothed.astype(bf16)
        retain = jax.nn.sigmoid(jnp.dot(rounded, md[...], preferred_element_type=f32))
        admit = jax.nn.sigmoid(jnp.dot(rounded, mi[...], preferred_element_type=f32))
        log_decay = rate * retain + jump[first : first + count, :]
        decay = jnp.exp(log_decay)
        inflow = jnp.sqrt(expm1_negated(2.0 * log_decay)) * admit * rounded.astype(f32)
        for n in range(n_tiles):
            used = min(tile, rw - n * tile)
            dbuf[n, first : first + count, :used] = decay[:, n * tile : n * tile + used]
            ibuf[n, first : first + count, :used] = inflow[:, n * tile : n * tile + used]

    early = 16
    gates(early, length - early)
    b_part(10, 13)()
    take_edge(0, ext_r, r_pad)
    gates(0, early)
    seg = length // SEGS

    def scan_step(j, carry):
        new = []
        for n, (p, s) in enumerate(carry):
            at = (n, pl.ds(j, SEGS, stride=seg), slice(None))
            d, i = dbuf[at], ibuf[at]
            p, s = d * p, d * s + i
            dbuf[at] = p
            ibuf[at] = s
            new.append((p, s))
        return tuple(new)

    start = tuple((jnp.ones((SEGS, tile), f32), jnp.zeros((SEGS, tile), f32)) for _ in range(n_tiles))
    ends = lax.fori_loop(0, seg, scan_step, start)
    p_all = jnp.concatenate([e[0] for e in ends], axis=1)
    s_all = jnp.concatenate([e[1] for e in ends], axis=1)
    half = cy.shape[2] // 2
    p_run, s_run = jnp.ones((1, half), f32), jnp.zeros((1, half), f32)
    before = []
    for g in range(SEGS):
        before.append((p_run, s_run))
        p_g, s_g = p_all[g : g + 1, :], s_all[g : g + 1, :]
        p_run, s_run = p_run * p_g, p_g * s_run + s_g

    def carry_copy(buf, slot, send, recv, to):
        return pltpu.make_async_remote_copy(
            src_ref=buf.at[slot], dst_ref=buf.at[slot], send_sem=send.at[0], recv_sem=recv.at[0],
            device_id={"sp": rem(to[0], NZ) * NY + rem(to[1], NY)}, device_id_type=MESH,
        )

    cy[y, :, :half] = p_run
    cy[y, :, half:] = s_run
    for d in range(1, NY):
        carry_copy(cy, pl.ds(y, 1), cy_s, cy_r, (z, y + d)).start()
    for k in groups_of(HALF):
        g_in.along_y(k)
    for k in groups_of(HALF - 1) + groups_of(HALF):
        g_in.along_y_last(k)
    b_part(13, NZ)()
    conv_val = acc_b[:, :cw].astype(bf16).astype(f32)
    conv_gate = acc_b[:, cw : 2 * cw].astype(bf16).astype(f32)
    ext_c[c_pad:, :] = (conv_val * jax.nn.sigmoid(conv_gate)).astype(bf16).astype(f32)
    edges[1].start()
    gate = jnp.concatenate([acc_a[:, rw:], acc_b[:, 2 * cw :]], axis=1).astype(bf16).astype(f32)
    gbuf[...] = 0.5 * gate * (1.0 + jnp.tanh(0.7978845608028654 * (gate + 0.044715 * gate * gate * gate)))
    out_step(HALF + 1 - lag)
    carry_copy(cy, pl.ds(0, NY - 1), cy_s, cy_r, (z, y + 1)).wait_recv()
    p_run, s_run = jnp.ones((1, half), f32), jnp.zeros((1, half), f32)
    p_mine, s_mine = p_run, s_run
    for n in range(NY):
        p_mine = jnp.where(y == n, p_run, p_mine)
        s_mine = jnp.where(y == n, s_run, s_mine)
        p_n, s_n = cy[n, :, :half], cy[n, :, half:]
        p_run, s_run = p_run * p_n, p_n * s_run + s_n
    cz[z, :, :half] = p_run
    cz[z, :, half:] = s_run
    for d in range(1, NZ):
        carry_copy(cz, pl.ds(z, 1), cz_s, cz_r, (z + d, y)).start()
    out_step(HALF + 2 - lag)
    n_taps = taps.shape[0]
    wide = taps[...].astype(f32)
    tap_rows = 32

    def filter_rows(first):
        total = jnp.broadcast_to(bias[...], (tap_rows, cw))
        for k in range(n_taps):
            at = first + c_pad - (n_taps - 1) + k
            total = total + wide[k : k + 1, :] * ext_c[at : at + tap_rows, :]
        filt[first : first + tap_rows, :] = total

    for i in range(1, length // tap_rows):
        filter_rows(i * tap_rows)
    take_edge(1, ext_c, c_pad)
    filter_rows(0)
    filtered = filt[...]
    row_id = lax.broadcasted_iota(jnp.int32, (8, cw), 0)
    first_half = jnp.where(row_id < 4, 1.0, 0.0)
    exact = lax.Precision.HIGHEST
    stats[tp] = lax.dot_general(
        first_half, filtered, NT_DIMS, precision=exact, preferred_element_type=f32
    ) + lax.dot_general(
        1.0 - first_half, filtered * filtered, NT_DIMS, precision=exact, preferred_element_type=f32
    )

    def stat_copy(d):
        return pltpu.make_async_remote_copy(
            src_ref=stats.at[tp], dst_ref=stats.at[tp], send_sem=stat_s.at[0], recv_sem=stat_r.at[0],
            device_id={"tp": rem(tp + d, NX * NC)}, device_id_type=MESH,
        )

    stats_of_others = pltpu.make_async_remote_copy(
        src_ref=stats.at[pl.ds(0, NX * NC - 1)], dst_ref=stats.at[pl.ds(0, NX * NC - 1)],
        send_sem=stat_s.at[0], recv_sem=stat_r.at[0],
        device_id={"tp": rem(tp + 1, NX * NC)}, device_id_type=MESH,
    )

    for d in range(1, NX * NC):
        stat_copy(d).start()

    out_step(HALF + 3 - lag)
    stats_of_others.wait_recv()
    totals = stats[0]
    for n in range(1, NX * NC):
        totals = totals + stats[n]
    scale = 1.0 / CONV_WIDTH
    row_id = lax.broadcasted_iota(jnp.int32, (8, cw), 0)
    mean = lax.dot_general(
        totals * scale, jnp.where(row_id == 0, 1.0, 0.0), TN_DIMS, precision=exact, preferred_element_type=f32
    )
    square = lax.dot_general(
        totals * scale, jnp.where(row_id == 4, 1.0, 0.0), TN_DIMS, precision=exact, preferred_element_type=f32
    )
    spread = jnp.maximum(square - mean * mean, 0.0)
    scaled = (filt[...] - mean) * lax.rsqrt(spread + 1e-05) * cgain[...]
    co[...] = (scaled * jax.nn.sigmoid(scaled)).astype(bf16)
    out_step(HALF + 4 - lag)
    out_step(HALF + 5 - lag)
    for s in range(max(HALF + 6 - lag, 0), HALF + 3):
        out_step(s)
    carry_copy(cz, pl.ds(0, NZ - 1), cz_s, cz_r, (z + 1, y)).wait_recv()
    entering = jnp.zeros((1, half), f32)
    for n in range(NZ):
        entering = jnp.where(n < z, cz[n, :, :half] * entering + cz[n, :, half:], entering)
    entering = p_mine * entering + s_mine
    for g, (p_g, s_g) in enumerate(before):
        part = slice(g * seg, (g + 1) * seg)
        at_start = p_g * entering + s_g
        for n in range(n_tiles):
            used = min(tile, rw - n * tile)
            lanes = slice(n * tile, n * tile + used)
            state = ibuf[n, part, :used] + dbuf[n, part, :used] * at_start[:, lanes]
            ro[part, lanes] = (gbuf[part, lanes] * state).astype(bf16)

    def chip_rows(xx, cc):
        return pl.ds(pl.multiple_of((rem(xx, NX) * NC + rem(cc, NC)) * n_tok, n_tok), n_tok)

    block = 512

    def out_part(j, carry):
        cols = pl.ds(pl.multiple_of(j * block, block), block)
        pc[:, cols] = lax.dot_general(
            co[...], oc[cols, :], NT_DIMS, preferred_element_type=f32
        ) + lax.dot_general(ro[...], orr[cols, :rw], NT_DIMS, preferred_element_type=f32)
        for d in range(NX):
            ps[d, :, cols] = pc[chip_rows(x + d, c + 1), cols].astype(bf16)
        return carry

    quarter = width // 4

    def lanes_of(q):
        return slice(q * quarter, (q + 1) * quarter)

    def pair_copy(d, q):
        lanes = lanes_of(q)
        return pltpu.make_async_remote_copy(
            src_ref=ps.at[d, :, lanes], dst_ref=pr.at[d, :, lanes],
            send_sem=pr_s.at[0], recv_sem=pr_r.at[4 * d + q],
            device_id={"tp": x * NC + rem(c + 1, NC)}, device_id_type=MESH,
        )

    def project(q):
        n_blocks = quarter // block
        lax.fori_loop(q * n_blocks, (q + 1) * n_blocks, out_part, 0)
        for d in (2, 1, 3, 0):
            pair_copy(d, q).start()

    def x_copy(src, dst, index, q, xx):
        return pltpu.make_async_remote_copy(
            src_ref=src.at[:, lanes_of(q)], dst_ref=dst.at[:, lanes_of(q)],
            send_sem=x_s.at[index // 4], recv_sem=x_r.at[index],
            device_id={"tp": rem(xx, NX) * NC + c}, device_id_type=MESH,
        )

    def chip_sum(d, q):
        pair_copy(d, q).wait_recv()
        return pc[chip_rows(x + d, c), lanes_of(q)] + pr[d, :, lanes_of(q)].astype(f32)

    far = [x_copy(s2, two, q, q, x + 1 if q < 2 else x - 1) for q in range(4)]
    up = [x_copy(sp_buf, from_m, 4 + q, q, x + 1) for q in range(4)]
    down = [x_copy(sm_buf, from_p, 8 + q, q, x - 1) for q in range(4)]

    def send_far(q):
        s2[:, lanes_of(q)] = chip_sum(2, q).astype(bf16)
        far[q].start()

    def send_near(d, q):
        buf, copies = (sp_buf, up) if d == 1 else (sm_buf, down)
        total = chip_sum(d, q)
        if (q < 2) == (d == 1):
            far[q].wait_recv()
            total = total + two[:, lanes_of(q)].astype(f32)
        buf[:, lanes_of(q)] = total.astype(bf16)
        copies[q].start()

    project(0)
    project(2)
    send_far(0)
    send_far(2)
    project(1)
    project(3)
    send_near(3, 0)
    send_near(1, 2)
    send_far(1)
    send_far(3)
    send_near(3, 1)
    send_near(1, 3)
    send_near(1, 0)
    send_near(3, 2)
    send_near(1, 1)
    send_near(3, 3)
    mine = chip_rows(x, c)
    for q in range(4):
        pc[mine, lanes_of(q)] = chip_sum(0, q)
    for q in (0, 2, 1, 3):
        at = lanes_of(q)
        up[q].wait_recv()
        down[q].wait_recv()
        out[:, at] = (pc[mine, at] + (from_m[:, at].astype(f32) + from_p[:, at].astype(f32))).astype(bf16)

    g_in.finish()
    g_out.finish()
    tok_copy(nt.at[pl.ds(0, 7 * n_tok)], 0, x + 1, c).wait_send()
    for e in edges:
        e.wait_send()
    stats_of_others.wait_send()
    carry_copy(cy, pl.ds(0, NY - 1), cy_s, cy_r, (z, y + 1)).wait_send()
    carry_copy(cz, pl.ds(0, NZ - 1), cz_s, cz_r, (z + 1, y)).wait_send()
    pltpu.make_async_remote_copy(
        src_ref=ps, dst_ref=pr, send_sem=pr_s.at[0], recv_sem=pr_r.at[0],
        device_id={"tp": x * NC + rem(c + 1, NC)}, device_id_type=MESH,
    ).wait_send()
    for n, buf in enumerate((s2, sp_buf, sm_buf)):
        pltpu.make_async_remote_copy(
            src_ref=buf, dst_ref=two, send_sem=x_s.at[n], recv_sem=x_r.at[0],
            device_id={"tp": rem(x + 1, NX) * NC + c}, device_id_type=MESH,
        ).wait_send()


def shards(
    tokens, norm_gain, conv_val_w, conv_gate_w, rec_gate_w, rec_in_w, conv_taps, conv_bias, conv_gain,
    short_taps, decay_map, input_map, decay_base, decay_jump, out_conv_w, out_rec_w,
):
    cw, rw = conv_val_w.shape[1], rec_in_w.shape[1]
    n_tok, width = tokens.shape
    length = n_tok * NX * NC
    wide = rw + -rw % 128
    f32, bf16 = jnp.float32, jnp.bfloat16
    vmem = pl.BlockSpec(memory_space=pltpu.VMEM)
    V, S = pltpu.VMEM, pltpu.SemaphoreType.DMA
    given = (
        tokens,
        norm_gain[None, :],
        conv_val_w,
        conv_gate_w,
        rec_in_w,
        rec_gate_w,
        out_conv_w.T,
        out_rec_w.T,
        conv_taps,
        conv_bias[None, :],
        conv_gain[None, :],
        short_taps,
        decay_map,
        input_map,
        decay_base[None, :],
        decay_jump.T,
    )
    return pl.pallas_call(
        whole_kernel,
        out_shape=pltpu.VMEM((n_tok, width), bf16),
        in_specs=[pl.BlockSpec(memory_space=pltpu.HBM)] * 16,
        out_specs=vmem,
        scratch_shapes=[
            *(V(g.shape, g.dtype) for g in given),
            S((16,)),
            V((length, width), bf16),
            V((width, 2 * cw), bf16),
            V((width, 2 * rw), bf16),
            V((length, 2 * cw), f32),
            V((length, 2 * rw), f32),
            V((width, cw), bf16),
            V((width * 3 // 2, 128), bf16),
            V((width, wide), bf16),
            V((length + 32, cw), f32),
            V((length + 8, rw), f32),
            V((length, cw), f32),
            V((rw, rw), bf16),
            V((rw, rw), bf16),
            V((NX * NC, 8, length), f32),
            V((wide // 128, length, 128), f32),
            V((wide // 128, length, 128), f32),
            V((length, rw), f32),
            V((length, cw), bf16),
            V((length, rw), bf16),
            V((length, rw), f32),
            V((NY, 1, 2 * wide), f32),
            V((NZ, 1, 2 * wide), f32),
            V((length, width), f32),
            V((NX, n_tok, width), bf16),
            V((NX, n_tok, width), bf16),
            V((n_tok, width), bf16),
            V((n_tok, width), bf16),
            V((n_tok, width), bf16),
            V((n_tok, width), bf16),
            V((n_tok, width), bf16),
            V((n_tok, width), bf16),
            *Gather.semaphores(),
            *Gather.semaphores(),
            S((1,)), S((9,)), S((2,)), S((2,)), S((1,)), S((1,)), S((1,)), S((1,)),
            S((1,)), S((1,)), S((1,)), S((4 * NX,)), S((3,)), S((12,)),
        ],
        compiler_params=pltpu.CompilerParams(
            collective_id=0, has_side_effects=True, vmem_limit_bytes=66_640_000
        ),
    )(*given)


def solution(mesh):
    in_specs = (
        P(("sp", "tp"), None), P(), P("sp", "tp"), P("sp", "tp"), P("sp", "tp"), P("sp", "tp"),
        P(None, "tp"), P("tp"), P("tp"), P(None, "tp"), P("tp", None, None), P("tp", None, None),
        P("tp"), P("sp", "tp"), P("tp", "sp"), P("tp", "sp"),
    )
    return jax.shard_map(
        shards, mesh=mesh, in_specs=in_specs, out_specs=P(("sp", "tp"), None), check_vma=False
    )
```
